128 devices in a mesh: rep: 2 (over z_hi), fs: 32 (over z_lo, y, x), tp: 2 (over core).
Axes of the slice: x: 4, y: 4, z: 4 (z_hi: 2, z_lo: 2; z = z_hi * 2 + z_lo), core: 2. Of those that a mesh axis runs over, the one named last changes fastest.
Arguments:
- layer_in: bfloat16 [65536, 2048], P(('rep', 'fs'), 'tp'), may hold values from -60 to 60
- mix_gain: bfloat16 [2048], P('tp'), may hold values from 0.099609375 to 1.8984375
- pool_weight: float32 [4, 512, 512], P('tp', None, 'fs'), may hold values from -0.25 to 0.25
- pool_scale: float32 [4, 512], P('tp'), may hold values from 0.1 to 1.9
- out_weight: float32 [2048, 2048], P('tp', 'fs'), may hold values from -0.125 to 0.125
- out_scale: float32 [2048], P('tp'), may hold values from 0.1 to 1.9
- channel_gain: bfloat16 [2048], P('tp'), may hold values from 0.099609375 to 1.8984375
- up_weight: float32 [2048, 2816], P('fs', 'tp'), may hold values from -0.125 to 0.125
- up_scale: float32 [2816], P('tp'), may hold values from 0.1 to 1.9
- gate_weight: float32 [2048, 2816], P('fs', 'tp'), may hold values from -0.125 to 0.125
- gate_scale: float32 [2816], P('tp'), may hold values from 0.1 to 1.9
- conv_weight: float32 [3, 2816], P(None, 'tp'), may hold values from -3 to 3
- down_weight: float32 [2816, 2048], P('tp', 'fs'), may hold values from -0.109375 to 0.109375
- down_scale: float32 [2048], P('tp'), may hold values from 0.1 to 1.9
Outputs:
- layer_out: bfloat16 [65536, 2048], P(('rep', 'fs'), 'tp')
The draws below stay inside these ranges and needn't reach their ends.
All inputs are finite; a program needn't handle non-finite values.
Results may differ from the reference program's by a relative error of at most 0.0095.
Values may be sent and summed in bfloat16 or wider, within the bound.
A program may use at most 128 MiB of HBM per device.

```python
import jax
import jax.numpy as jnp
from jax import lax

D = 2048
FF = 2816
GROUPS = 4
GROUP_DIM = 512
LENGTH = 256
TOKENS = 65536
N_FS = 32
N_TP = 2


def draw_layer_in(key, part):
    first, second, third = jax.random.split(jax.random.fold_in(key, 11), 3)
    rising = jnp.exp(jnp.log(3.0) * jnp.arange(D, dtype=jnp.float32) / D)
    column = rising * jax.random.uniform(second, (D,), jnp.float32, 0.5, 1.5)
    base = jnp.clip(jax.random.normal(first, (TOKENS, D), jnp.float32), -4.0, 4.0)
    row_scale = jnp.exp(jax.random.uniform(third, (TOKENS, 1), jnp.float32, jnp.log(0.3), jnp.log(3.0)))
    return (base * column[None] * row_scale).astype(jnp.bfloat16)


def block_scale(stream_key, extent, shards, low, top_value):
    def one(dim, parts):
        heights = jax.random.uniform(jax.random.fold_in(jax.random.fold_in(stream_key, 6), dim), (parts,), jnp.float32, low / len(shards), top_value / len(shards))
        return jnp.repeat(jnp.exp(heights), extent[dim] // parts).reshape((-1,) + (1,) * (len(extent) - dim - 1))

    level = one(*shards[0])
    for cut in shards[1:]:
        level = level * one(*cut)
    return level


def bell_draw(own_key, shape, spread, reach, cuts=(), kind=jnp.bfloat16):
    factor_of = block_scale(own_key, shape, cuts, -0.22, 0.18) if cuts else 1.0
    values = jax.random.normal(own_key, shape, jnp.float32) * spread * factor_of
    return jnp.minimum(jnp.maximum(values, -reach), reach).astype(kind)


def setup_inputs(seed: int = 0) -> dict:
    arg_keys = jax.random.split(jax.random.key(seed), 15)
    layer_in = draw_layer_in(jax.random.fold_in(arg_keys[14], 71), 0)
    mix_gain = jnp.clip(1.0 + 0.18 * jax.random.normal(arg_keys[1], (D,), jnp.float32), 0.099609375, 1.8984375).astype(jnp.bfloat16)
    pool_weight = bell_draw(arg_keys[2], (GROUPS, GROUP_DIM, GROUP_DIM), GROUP_DIM ** -0.5, 0.25, ((0, 2), (2, 32)), jnp.float32)
    pool_scale = jnp.clip(1.0 + 0.18 * jax.random.normal(arg_keys[3], (GROUPS, GROUP_DIM), jnp.float32), 0.1, 1.9)
    out_weight = bell_draw(arg_keys[4], (D, D), D ** -0.5, 0.125, ((0, 2), (1, 32)), jnp.float32)
    out_scale = jnp.clip(1.0 + 0.18 * jax.random.normal(arg_keys[5], (D,), jnp.float32), 0.1, 1.9)
    channel_gain = jnp.clip(1.0 + 0.18 * jax.random.normal(arg_keys[6], (D,), jnp.float32), 0.099609375, 1.8984375).astype(jnp.bfloat16)
    up_weight = bell_draw(arg_keys[7], (D, FF), D ** -0.5, 0.125, ((0, 32), (1, 2)), jnp.float32)
    up_scale = jnp.clip(1.0 + 0.18 * jax.random.normal(arg_keys[8], (FF,), jnp.float32), 0.1, 1.9)
    gate_weight = bell_draw(arg_keys[9], (D, FF), D ** -0.5, 0.125, ((0, 32), (1, 2)), jnp.float32)
    gate_scale = jnp.clip(1.0 + 0.18 * jax.random.normal(arg_keys[10], (FF,), jnp.float32), 0.1, 1.9)
    conv_weight = bell_draw(arg_keys[11], (3, FF), 0.577, 3.0, ((1, 2),), jnp.float32)
    down_weight = bell_draw(arg_keys[12], (FF, D), FF ** -0.5, 0.109375, ((0, 2), (1, 32)), jnp.float32)
    down_scale = jnp.clip(1.0 + 0.18 * jax.random.normal(arg_keys[13], (D,), jnp.float32), 0.1, 1.9)
    return dict(layer_in=layer_in, mix_gain=mix_gain, pool_weight=pool_weight, pool_scale=pool_scale, out_weight=out_weight, out_scale=out_scale, channel_gain=channel_gain, up_weight=up_weight, up_scale=up_scale, gate_weight=gate_weight, gate_scale=gate_scale, conv_weight=conv_weight, down_weight=down_weight, down_scale=down_scale)


EPS = 1e-06

def settle(values):
    return lax.optimization_barrier(values.astype(jnp.bfloat16)).astype(jnp.float32)

def band_table(length, window):
    rows = lax.broadcasted_iota(jnp.int32, (length, length), 0)
    cols = lax.broadcasted_iota(jnp.int32, (length, length), 1)
    lower = jnp.maximum(rows - window // 2, 0)
    upper = jnp.minimum(rows - window // 2 + window, length)
    inside = (cols >= lower) & (cols < upper)
    count = (upper[:, :1] - lower[:, :1]).astype(jnp.float32)
    return (inside.astype(jnp.bfloat16), count)

def partial_sums(left, right):
    part = left.shape[1] // N_TP
    total = jnp.zeros((left.shape[0], right.shape[1]), jnp.float32)
    for index in range(N_TP):
        piece = jnp.dot(left[:, index * part:(index + 1) * part], right[index * part:(index + 1) * part], preferred_element_type=jnp.float32)
        total = total + settle(piece)
    return total

def block_layer(block_in, mix_gain, pool_bf, pool_scale, out_bf, out_scale, channel_gain, up_bf, up_scale, gate_bf, gate_scale, conv_weight, down_bf, down_scale):
    rows = block_in.shape[0]
    seqs = rows // LENGTH
    x32 = block_in.astype(jnp.float32)
    normed = settle(x32 * lax.rsqrt(lax.optimization_barrier(jnp.mean(x32 * x32, axis=1, keepdims=True)) + EPS) * mix_gain.astype(jnp.float32))
    grouped_in = normed.reshape(seqs, LENGTH, GROUPS, GROUP_DIM)
    outputs = []
    for group in range(GROUPS):
        band, count = band_table(LENGTH, 2 ** (group + 1))
        piece = grouped_in[:, :, group, :]
        total = jnp.einsum('ij,sjc->sic', band.astype(jnp.float32), piece)
        outputs.append(settle(total / count[None] - piece))
    pooled = jnp.stack(outputs, axis=2)
    grouped = jnp.einsum('slgc,gcd->slgd', pooled, pool_bf.astype(jnp.float32)) * pool_scale[None, None]
    grouped = settle(grouped).astype(jnp.bfloat16).reshape(rows, D)
    mixer_sum = partial_sums(grouped, out_bf)
    middle = (x32 + mixer_sum * out_scale[None]).astype(jnp.bfloat16)
    m32 = middle.astype(jnp.float32)
    chan_normed = (m32 * lax.rsqrt(lax.optimization_barrier(jnp.mean(m32 * m32, axis=1, keepdims=True)) + EPS) * channel_gain.astype(jnp.float32)).astype(jnp.bfloat16)
    lifted = settle(jnp.dot(chan_normed, up_bf, preferred_element_type=jnp.float32) * up_scale[None])
    gated = jnp.dot(chan_normed, gate_bf, preferred_element_type=jnp.float32) * gate_scale[None]
    padded = jnp.pad(lifted.reshape(seqs, LENGTH, FF), ((0, 0), (1, 1), (0, 0)))
    conv = conv_weight[0] * padded[:, :-2] + conv_weight[1] * padded[:, 1:-1] + conv_weight[2] * padded[:, 2:]
    hidden = (jax.nn.gelu(conv).reshape(rows, FF) * gated).astype(jnp.bfloat16)
    chan_sum = partial_sums(hidden, down_bf)
    return (m32 + chan_sum * down_scale[None]).astype(jnp.bfloat16)

def reference(layer_in, mix_gain, pool_weight, pool_scale, out_weight, out_scale, channel_gain, up_weight, up_scale, gate_weight, gate_scale, conv_weight, down_weight, down_scale):
    pool_bf = pool_weight.astype(jnp.bfloat16)
    out_bf = out_weight.astype(jnp.bfloat16)
    up_bf = up_weight.astype(jnp.bfloat16)
    gate_bf = gate_weight.astype(jnp.bfloat16)
    down_bf = down_weight.astype(jnp.bfloat16)
    blocks = layer_in.reshape(N_FS, TOKENS // N_FS, D)

    def one_block(block_in):
        return block_layer(block_in, mix_gain, pool_bf, pool_scale, out_bf, out_scale, channel_gain, up_bf, up_scale, gate_bf, gate_scale, conv_weight, down_bf, down_scale)
    return lax.map(one_block, blocks).reshape(TOKENS, D)
```

```python
import functools

import jax
import jax.numpy as jnp
from jax import lax
from jax.experimental import pallas as pl
from jax.experimental.pallas import tpu as pltpu
from jax.sharding import Mesh
from jax.sharding import PartitionSpec as P

LENGTH = 256
FS = ("fs_0", "fs_1", "fs_2")
REP_FS = ("rep", "fs_0", "fs_1", "fs_2")
EPS = 1e-06

F32 = jnp.float32
BF16 = jnp.bfloat16
MESH = pl.DeviceIdType.MESH

ROWS = 1024
HALF = 1024
WIDTH = 2048
HID = 1408
SEQS = ROWS // LENGTH
LANES = 128

U_POOL = 0
U_OUT = 2
U_LAST = 10
U_FF = 12
U_DOWN = 32
UNITS = 43
COLOURS = 4
CHUNKS = 11
STAGES = 5
SLOTS = CHUNKS + STAGES

ORDERS = (("x", "y", "z"), ("y", "x", "z"), ("x", "z", "y"), ("y", "z", "x"))
STEPS = (
    ((0, "a"), (0, "b"), (1, "a"), (1, "b"), (2, "a")),
    ((0, "a"), (0, "b"), (1, "a"), (1, "b"), (2, "a")),
    ((0, "a"), (0, "b"), (1, "a"), (2, "a"), (2, "b")),
    ((0, "a"), (0, "b"), (1, "a"), (2, "a"), (2, "b")),
)
AXIS = {"x": "fs_2", "y": "fs_1"}


def dot_nt(left, right):
    return lax.dot_general(left, right, (((1,), (1,)), ((), ())), preferred_element_type=F32)


def kernel(
    x_hbm,
    pool_hbm,
    out_hbm,
    up_hbm,
    gate_hbm,
    down_hbm,
    prm_hbm,
    ffp_hbm,
    y_hbm,
    w,
    x,
    mixed,
    give,
    got,
    own,
    mid,
    normed,
    hid,
    acc,
    st_pool,
    st_out,
    st_up,
    st_gate,
    st_down,
    prm,
    ffp,
    sq,
    in_sem,
    send_sem,
    recv_sem,
    tp_send,
    tp_recv,
    y_sem,
):
    rep = lax.axis_index("rep")
    zl = lax.axis_index("fs_0")
    me = {"z": zl, "y": lax.axis_index("fs_1"), "x": lax.axis_index("fs_2")}
    tp = lax.axis_index("tp")
    mate = 1 - tp
    zz = rep * 2 + zl
    z_up = lax.rem(zz + 1, 4)
    z_down = lax.rem(zz + 3, 4)

    def to_z(place):
        return {"rep": place // 2, "fs_0": lax.rem(place, 2)}

    def ring(dim, shift):
        return lax.rem(me[dim] + shift + 4, 4)

    peers = [to_z(z_up), to_z(z_down), {"tp": mate}]
    for dim in ("x", "y"):
        peers += [{AXIS[dim]: ring(dim, 1)}, {AXIS[dim]: ring(dim, -1)}]

    loads = [
        pltpu.make_async_copy(src, dst, in_sem.at[k])
        for k, (src, dst) in enumerate(
            (
                (pool_hbm, st_pool),
                (out_hbm, st_out),
                (up_hbm, st_up),
                (gate_hbm, st_gate),
                (down_hbm, st_down),
                (x_hbm, x),
                (prm_hbm, prm.at[tp]),
                (ffp_hbm, ffp),
            )
        )
    ]
    for load in loads:
        load.start()

    barrier = pltpu.get_barrier_semaphore()
    for peer in peers:
        pl.semaphore_signal(barrier, inc=1, device_id=peer, device_id_type=MESH)

    for load in loads:
        load.wait()

    mine = (me["z"], me["y"], me["x"])
    for g in range(2):
        for ct in range(4):
            block = st_pool[g, ct * LANES : (ct + 1) * LANES, :]
            w[(U_POOL + g, *mine, pl.ds(ct * 16, 16), slice(None))] = block.T.astype(BF16)
    for k in range(8):
        w[(U_OUT + k, *mine)] = st_out[k * LANES : (k + 1) * LANES, :].T.astype(BF16)
    for k in range(11):
        w[(U_DOWN + k, *mine)] = st_down[k * LANES : (k + 1) * LANES, :].T.astype(BF16)
        columns = slice(k * LANES, (k + 1) * LANES)
        at_up = U_LAST if k == 10 else U_FF + 4 * (k // 2) + k % 2
        at_gate = U_LAST + 1 if k == 10 else U_FF + 4 * (k // 2) + 2 + k % 2
        w[(at_up, *mine)] = st_up[:, columns].astype(BF16)
        w[(at_gate, *mine)] = st_gate[:, columns].astype(BF16)

    pl.semaphore_wait(barrier, len(peers))

    def across(src, dst, index):
        return pltpu.make_async_remote_copy(
            src_ref=src,
            dst_ref=dst,
            send_sem=tp_send.at[index],
            recv_sem=tp_recv.at[index],
            device_id={"tp": mate},
            device_id_type=MESH,
        )

    across(prm_hbm, prm.at[tp], 0).start()

    def region(u, order, phase, place, rows):
        picks = {}
        for k, dim in enumerate(order):
            if k < phase:
                picks[dim] = slice(None)
            elif k == phase:
                picks[dim] = pl.ds(place, 1)
            else:
                picks[dim] = pl.ds(me[dim], 1)
        return w.at[u, picks["z"], picks["y"], picks["x"], rows, :]

    every, first, second = pl.ds(0, 64), pl.ds(0, 32), pl.ds(32, 32)

    def moves(colour, stage):
        order = ORDERS[colour]
        phase, step = STEPS[colour][stage]
        dim = order[phase]
        if dim == "z":
            there = 1 - zl
            return phase, (
                (zl, first, to_z(z_up), there, first),
                (zl, second, to_z(z_down), there, second),
            )
        right, left = {AXIS[dim]: ring(dim, 1)}, {AXIS[dim]: ring(dim, -1)}
        if step == "a":
            return phase, (
                (me[dim], every, right, ring(dim, -1), every),
                (me[dim], every, left, ring(dim, 1), every),
            )
        return phase, (
            (ring(dim, -1), first, right, ring(dim, 2), first),
            (ring(dim, 1), second, left, ring(dim, 2), second),
        )

    def hop(colour, stage, chunk, direction, arriving):
        u = chunk * COLOURS + colour
        phase, both = moves(colour, stage)
        place, rows, peer, from_place, from_rows = both[direction]
        if arriving:
            place, rows = from_place, from_rows
        ref = region(u, ORDERS[colour], phase, place, rows)
        return pltpu.make_async_remote_copy(
            src_ref=ref,
            dst_ref=ref,
            send_sem=send_sem.at[u],
            recv_sem=recv_sem.at[u, stage, direction],
            device_id=peer,
            device_id_type=MESH,
        )

    def advance(colour, slot):
        for depth in (0, 5, 4, 3, 2, 1):
            chunk = slot - depth

            @pl.when((chunk >= 0) & (chunk * COLOURS + colour < UNITS))
            def _():
                if depth > 0:
                    for direction in range(2):
                        hop(colour, depth - 1, chunk, direction, True).wait_recv()
                if depth < STAGES:
                    for direction in range(2):
                        hop(colour, depth, chunk, direction, False).start()

    def rows_of(s):
        return pl.ds(pl.multiple_of(s * LENGTH, LENGTH), LENGTH)

    def squares():
        def one(s, _):
            part = x[rows_of(s), :].astype(F32)
            total = jnp.sum(part * part, axis=1, keepdims=True)
            sq[tp, rows_of(s), :] = jnp.broadcast_to(total, (LENGTH, LANES))
            return 0

        lax.fori_loop(0, SEQS, one, 0)

    def pool(s):
        total = sq[0, rows_of(s), :] + sq[1, rows_of(s), :]
        scale = lax.rsqrt(total / WIDTH + EPS)[:, :1]
        at = lax.broadcasted_iota(jnp.int32, (LENGTH, LENGTH), 0)
        col = lax.broadcasted_iota(jnp.int32, (LENGTH, LENGTH), 1)
        for g in range(2):
            reach = jnp.where(tp == 0, 1 << g, 4 << g)
            lower = jnp.maximum(at - reach, 0)
            upper = jnp.minimum(at + reach, LENGTH)
            band = jnp.where((col >= lower) & (col < upper), 1.0, 0.0).astype(BF16)
            count = (upper[:, :1] - lower[:, :1]).astype(F32)
            columns = slice(g * 512, (g + 1) * 512)
            piece = x[rows_of(s), columns].astype(F32) * scale * prm[tp, 0:1, columns]
            piece = piece.astype(BF16)
            window = jnp.dot(band, piece, preferred_element_type=F32)
            mixed[rows_of(s), columns] = (window / count - piece.astype(F32)).astype(BF16)

    def group(s):
        for g in range(2):
            columns = slice(g * 512, (g + 1) * 512)
            maps = w[U_POOL + g].reshape(32, 4, 16, LANES)
            right = jnp.concatenate([maps[:, ct].reshape(512, LANES) for ct in range(4)], axis=1)
            out = dot_nt(mixed[rows_of(s), columns], right) * prm[tp, 4:5, columns]
            mixed[rows_of(s), columns] = out.astype(BF16)

    def project(side, block, dst):
        right = jnp.concatenate(
            [w[U_OUT + k, side, block].reshape(256, LANES) for k in range(8)], axis=1
        )
        columns = pl.ds(pl.multiple_of(block * 256, 256), 256)

        def one(s, _):
            dst[rows_of(s), columns] = dot_nt(mixed[rows_of(s), :], right).astype(BF16)
            return 0

        lax.fori_loop(0, SEQS, one, 0)

    def give_piece(block, index):
        columns = pl.ds(pl.multiple_of(block * 256, 256), 256)
        return across(give.at[:, columns], got.at[:, columns], index + block)

    def middle(s):
        total = own[rows_of(s), :].astype(F32) + got[rows_of(s), :].astype(F32)
        value = x[rows_of(s), :].astype(F32) + total * prm[tp, 1:2, :]
        mid[tp, rows_of(s), :] = value.astype(BF16)

    def mid_piece(s, side):
        ref = mid.at[side, rows_of(s), :]
        return across(ref, ref, 6 + s)

    def norm(s):
        left = mid[0, rows_of(s), :].astype(F32)
        right = mid[1, rows_of(s), :].astype(F32)
        total = jnp.sum(left * left + right * right, axis=1, keepdims=True)
        scale = lax.rsqrt(total / WIDTH + EPS)
        normed[rows_of(s), 0:HALF] = (left * scale * prm[0, 2:3, :]).astype(BF16)
        normed[rows_of(s), HALF:WIDTH] = (right * scale * prm[1, 2:3, :]).astype(BF16)

    def hidden_of(up_raw, gate_raw, columns):
        lifted = (up_raw * ffp[0:1, columns]).astype(BF16).astype(F32)
        at = lax.broadcasted_iota(jnp.int32, lifted.shape, 0)
        before = jnp.where(at == 0, 0.0, pltpu.roll(lifted, 1, 0))
        after = jnp.where(at == LENGTH - 1, 0.0, pltpu.roll(lifted, LENGTH - 1, 0))
        conv = (
            ffp[2:3, columns] * before + ffp[3:4, columns] * lifted + ffp[4:5, columns] * after
        )
        return (jax.nn.gelu(conv) * (gate_raw * ffp[1:2, columns])).astype(BF16)

    def pair(u):
        return jnp.concatenate(
            [w[u].reshape(WIDTH, LANES), w[u + 1].reshape(WIDTH, LANES)], axis=1
        )

    def feed(j, s):
        u = U_FF + 4 * j
        left = normed[rows_of(s), :]
        up_raw = jnp.dot(left, pair(u), preferred_element_type=F32)
        gate_raw = jnp.dot(left, pair(u + 2), preferred_element_type=F32)
        columns = pl.ds(pl.multiple_of(j * 256, 256), 256)
        hid[rows_of(s), columns] = hidden_of(up_raw, gate_raw, columns)

    def feed_last(s):
        both = jnp.dot(normed[rows_of(s), :], pair(U_LAST), preferred_element_type=F32)
        columns = pl.ds(10 * LANES, LANES)
        hid[rows_of(s), columns] = hidden_of(both[:, :LANES], both[:, LANES:], columns)

    def down_part(side, block, tiles):
        return jnp.concatenate(
            [w[U_DOWN + k, side, block].reshape(256, LANES) for k in tiles], axis=1
        )

    def down_first(s):
        def one(n, _):
            right = down_part(n // 4, lax.rem(n, 4), range(8))
            columns = pl.ds(pl.multiple_of(n * 256, 256), 256)
            acc[rows_of(s), columns] = dot_nt(hid[rows_of(s), 0:1024], right)
            return 0

        lax.fori_loop(0, 8, one, 0)

    def down_rest(side, block, dst):
        right = down_part(side, block, range(8, 11))
        wide = pl.ds(pl.multiple_of(side * HALF + block * 256, 256), 256)
        columns = pl.ds(pl.multiple_of(block * 256, 256), 256)

        def one(s, _):
            total = acc[rows_of(s), wide] + dot_nt(hid[rows_of(s), 1024:HID], right)
            dst[rows_of(s), columns] = total.astype(BF16)
            return 0

        lax.fori_loop(0, SEQS, one, 0)

    def compute(m):
        def during(start, count, body):
            @pl.when((m >= start) & (m < start + count))
            def _():
                body(m - start)

        def send_squares(_):
            squares()

        def start_squares(_):
            across(sq.at[tp], sq.at[tp], 1).start()

        def take_squares(_):
            across(sq.at[mate], sq.at[mate], 1).wait_recv()
            across(prm_hbm, prm.at[mate], 0).wait_recv()

        during(0, 1, send_squares)
        during(1, 1, start_squares)
        during(4, 1, take_squares)
        during(4, 4, pool)
        during(23, 4, group)

        def project_out(k):
            for part in range(2):
                project(mate, 2 * k + part, give)
                give_piece(2 * k + part, 2).start()

        def project_own(k):
            for part in range(2):
                project(tp, 2 * k + part, own)

        during(31, 2, project_out)
        during(33, 2, project_own)

        def take_mixer(_):
            for block in range(4):
                give_piece(block, 2).wait_recv()

        def middles(k):
            for part in range(2):
                middle(2 * k + part)
            for part in range(2):
                mid_piece(2 * k + part, tp).start()

        def norms(k):
            for part in range(2):
                mid_piece(2 * k + part, mate).wait_recv()
                norm(2 * k + part)

        during(35, 1, take_mixer)
        during(35, 2, middles)
        during(37, 2, norms)
        during(39, 20, lambda k: feed(k // 4, lax.rem(k, 4)))
        during(59, 4, feed_last)
        during(59, 4, down_first)

    def micro(m, _):
        slot, turn = m // COLOURS, lax.rem(m, COLOURS)
        for colour in range(COLOURS):

            @pl.when(turn == colour)
            def _():
                advance(colour, slot)

        compute(m)
        return 0

    lax.fori_loop(0, SLOTS * COLOURS, micro, 0)

    for block in range(4):
        give_piece(block, 2).wait_send()
    for block in range(4):
        down_rest(mate, block, give)
        give_piece(block, 10).start()
    for block in range(4):
        down_rest(tp, block, own)
    for block in range(4):
        give_piece(block, 10).wait_recv()

    def finish(s, _):
        total = own[rows_of(s), :].astype(F32) + got[rows_of(s), :].astype(F32)
        value = mid[tp, rows_of(s), :].astype(F32) + total * prm[tp, 3:4, :]
        x[rows_of(s), :] = value.astype(BF16)
        return 0

    lax.fori_loop(0, SEQS, finish, 0)
    result = pltpu.make_async_copy(x, y_hbm, y_sem)
    result.start()

    across(prm_hbm, prm.at[tp], 0).wait_send()
    across(sq.at[tp], sq.at[tp], 1).wait_send()
    for s in range(SEQS):
        mid_piece(s, tp).wait_send()
    for block in range(4):
        give_piece(block, 10).wait_send()

    def drain(u, _):
        same_size = normed.at[pl.ds(0, 31 * 32), pl.ds(0, 256)]
        pltpu.make_async_copy(same_size, same_size, send_sem.at[u]).wait()
        return 0

    lax.fori_loop(0, UNITS, drain, 0)
    result.wait()


def layer(
    layer_in,
    mix_gain,
    pool_weight,
    pool_scale,
    out_weight,
    out_scale,
    channel_gain,
    up_weight,
    up_scale,
    gate_weight,
    gate_scale,
    conv_weight,
    down_weight,
    down_scale,
):
    rows = [
        mix_gain.astype(F32),
        out_scale,
        channel_gain.astype(F32),
        down_scale,
        pool_scale.reshape(HALF),
    ]
    prm = jnp.pad(jnp.stack(rows), ((0, 3), (0, 0)))
    ffp = jnp.concatenate(
        [up_scale[None], gate_scale[None], conv_weight, jnp.zeros((3, HID), F32)], axis=0
    )
    anywhere = pl.BlockSpec(memory_space=pl.ANY)
    dma = pltpu.SemaphoreType.DMA
    return pl.pallas_call(
        kernel,
        out_shape=jax.ShapeDtypeStruct((ROWS, HALF), BF16),
        in_specs=[anywhere] * 8,
        out_specs=anywhere,
        scratch_shapes=[
            pltpu.VMEM((UNITS, 2, 4, 4, 64, LANES), BF16),
            pltpu.VMEM((ROWS, HALF), BF16),
            pltpu.VMEM((ROWS, HALF), BF16),
            pltpu.VMEM((ROWS, HALF), BF16),
            pltpu.VMEM((ROWS, HALF), BF16),
            pltpu.VMEM((ROWS, HALF), BF16),
            pltpu.VMEM((2, ROWS, HALF), BF16),
            pltpu.VMEM((ROWS, WIDTH), BF16),
            pltpu.VMEM((ROWS, HID), BF16),
            pltpu.VMEM((ROWS, WIDTH), F32),
            pltpu.VMEM((2, 512, 16), F32),
            pltpu.VMEM((1024, 64), F32),
            pltpu.VMEM((64, HID), F32),
            pltpu.VMEM((64, HID), F32),
            pltpu.VMEM((HID, 64), F32),
            pltpu.VMEM((2, 8, HALF), F32),
            pltpu.VMEM((8, HID), F32),
            pltpu.VMEM((2, ROWS, LANES), F32),
            dma((8,)),
            dma((UNITS,)),
            dma((UNITS, STAGES, 2)),
            dma((14,)),
            dma((14,)),
            dma,
        ],
        compiler_params=pltpu.CompilerParams(
            collective_id=0, has_side_effects=True, vmem_limit_bytes=66_000_000
        ),
    )(layer_in, pool_weight, out_weight, up_weight, gate_weight, down_weight, prm, ffp)


def solution(mesh):
    torus = Mesh(
        mesh.devices.reshape(mesh.shape["rep"], 2, 4, 4, mesh.shape["tp"]),
        ("rep", "fs_0", "fs_1", "fs_2", "tp"),
    )
    in_specs = (
        P(REP_FS, "tp"),
        P("tp"),
        P("tp", None, FS),
        P("tp", None),
        P("tp", FS),
        P("tp"),
        P("tp"),
        P(FS, "tp"),
        P("tp"),
        P(FS, "tp"),
        P("tp"),
        P(None, "tp"),
        P("tp", FS),
        P("tp"),
    )
    out_specs = P(REP_FS, "tp")
    return jax.shard_map(
        layer, mesh=torus, in_specs=in_specs, out_specs=out_specs, check_vma=False
    )
```

```python
import functools

import jax
import jax.numpy as jnp
from jax import lax
from jax.experimental import pallas as pl
from jax.experimental.pallas import tpu as pltpu
from jax.sharding import Mesh
from jax.sharding import PartitionSpec as P

LENGTH = 256
FS = ("fs_0", "fs_1", "fs_2")
REP_FS = ("rep", "fs_0", "fs_1", "fs_2")
EPS = 1e-06

F32 = jnp.float32
BF16 = jnp.bfloat16
MESH = pl.DeviceIdType.MESH

ROWS = 1024
HALF = 1024
WIDTH = 2048
HID = 1408
SEQS = ROWS // LENGTH
LANES = 128

U_POOL = 0
U_OUT = 2
U_LAST = 10
U_FF = 12
U_DOWN = 32
UNITS = 43
COLOURS = 4
CHUNKS = 11
STAGES = 5
SLOTS = CHUNKS + STAGES

ORDERS = (("x", "y", "z"), ("y", "x", "z"), ("x", "z", "y"), ("y", "z", "x"))
STEPS = (
    ((0, "a"), (0, "b"), (1, "a"), (1, "b"), (2, "a")),
    ((0, "a"), (0, "b"), (1, "a"), (1, "b"), (2, "a")),
    ((0, "a"), (0, "b"), (1, "a"), (2, "a"), (2, "b")),
    ((0, "a"), (0, "b"), (1, "a"), (2, "a"), (2, "b")),
)
AXIS = {"x": "fs_2", "y": "fs_1"}


def dot_nt(left, right):
    return lax.dot_general(left, right, (((1,), (1,)), ((), ())), preferred_element_type=F32)


def kernel(
    x_hbm,
    pool_hbm,
    out_hbm,
    up_hbm,
    gate_hbm,
    down_hbm,
    mix_gain_hbm,
    pool_scale_hbm,
    out_scale_hbm,
    gain_hbm,
    up_scale_hbm,
    gate_scale_hbm,
    conv_hbm,
    down_scale_hbm,
    y_hbm,
    w,
    x,
    mixed,
    give,
    got,
    own,
    mid,
    normed,
    hid,
    acc,
    st_pool,
    st_out,
    st_up,
    st_gate,
    st_down,
    mix_gain,
    pool_scale,
    out_scale,
    gain,
    mate_gain,
    up_scale,
    gate_scale,
    conv_taps,
    down_scale,
    sq,
    in_sem,
    send_sem,
    recv_sem,
    tp_send,
    tp_recv,
    y_sem,
):
    rep = lax.axis_index("rep")
    zl = lax.axis_index("fs_0")
    me = {"z": zl, "y": lax.axis_index("fs_1"), "x": lax.axis_index("fs_2")}
    tp = lax.axis_index("tp")
    mate = 1 - tp
    zz = rep * 2 + zl
    z_up = lax.rem(zz + 1, 4)
    z_down = lax.rem(zz + 3, 4)

    def to_z(place):
        return {"rep": place // 2, "fs_0": lax.rem(place, 2)}

    def ring(dim, shift):
        return lax.rem(me[dim] + shift + 4, 4)

    peers = [to_z(z_up), to_z(z_down), {"tp": mate}]
    for dim in ("x", "y"):
        peers += [{AXIS[dim]: ring(dim, 1)}, {AXIS[dim]: ring(dim, -1)}]

    loads = [
        pltpu.make_async_copy(src, dst, in_sem.at[k])
        for k, (src, dst) in enumerate(
            (
                (pool_hbm, st_pool),
                (out_hbm, st_out),
                (up_hbm, st_up),
                (gate_hbm, st_gate),
                (down_hbm, st_down),
                (x_hbm, x),
                (mix_gain_hbm, mix_gain),
                (pool_scale_hbm, pool_scale),
                (out_scale_hbm, out_scale),
                (gain_hbm, gain),
                (up_scale_hbm, up_scale),
                (gate_scale_hbm, gate_scale),
                (conv_hbm, conv_taps),
                (down_scale_hbm, down_scale),
            )
        )
    ]
    for load in loads:
        load.start()

    barrier = pltpu.get_barrier_semaphore()
    for peer in peers:
        pl.semaphore_signal(barrier, inc=1, device_id=peer, device_id_type=MESH)

    for load in loads:
        load.wait()

    mine = (me["z"], me["y"], me["x"])
    for g in range(2):
        for ct in range(4):
            block = st_pool[g, :, ct * LANES : (ct + 1) * LANES]
            w[(U_POOL + g, *mine, pl.ds(ct * 16, 16), slice(None))] = block.astype(BF16)
    for k in range(8):
        w[(U_OUT + k, *mine)] = st_out[:, k * LANES : (k + 1) * LANES].astype(BF16)
    for k in range(11):
        w[(U_DOWN + k, *mine)] = st_down[:, k * LANES : (k + 1) * LANES].astype(BF16)
        columns = slice(k * LANES, (k + 1) * LANES)
        at_up = U_LAST if k == 10 else U_FF + 4 * (k // 2) + k % 2
        at_gate = U_LAST + 1 if k == 10 else U_FF + 4 * (k // 2) + 2 + k % 2
        w[(at_up, *mine)] = st_up[:, columns].astype(BF16)
        w[(at_gate, *mine)] = st_gate[:, columns].astype(BF16)

    pl.semaphore_wait(barrier, len(peers))

    def across(src, dst, index):
        return pltpu.make_async_remote_copy(
            src_ref=src,
            dst_ref=dst,
            send_sem=tp_send.at[index],
            recv_sem=tp_recv.at[index],
            device_id={"tp": mate},
            device_id_type=MESH,
        )

    across(gain_hbm, mate_gain, 0).start()

    def region(u, order, phase, place, rows):
        picks = {}
        for k, dim in enumerate(order):
            if k < phase:
                picks[dim] = slice(None)
            elif k == phase:
                picks[dim] = pl.ds(place, 1)
            else:
                picks[dim] = pl.ds(me[dim], 1)
        return w.at[u, picks["z"], picks["y"], picks["x"], rows, :]

    every, first, second = pl.ds(0, 64), pl.ds(0, 32), pl.ds(32, 32)

    def moves(colour, stage):
        order = ORDERS[colour]
        phase, step = STEPS[colour][stage]
        dim = order[phase]
        if dim == "z":
            there = 1 - zl
            return phase, (
                (zl, first, to_z(z_up), there, first),
                (zl, second, to_z(z_down), there, second),
            )
        right, left = {AXIS[dim]: ring(dim, 1)}, {AXIS[dim]: ring(dim, -1)}
        if step == "a":
            return phase, (
                (me[dim], every, right, ring(dim, -1), every),
                (me[dim], every, left, ring(dim, 1), every),
            )
        return phase, (
            (ring(dim, -1), first, right, ring(dim, 2), first),
            (ring(dim, 1), second, left, ring(dim, 2), second),
        )

    def hop(colour, stage, chunk, direction, arriving):
        u = chunk * COLOURS + colour
        phase, both = moves(colour, stage)
        place, rows, peer, from_place, from_rows = both[direction]
        if arriving:
            place, rows = from_place, from_rows
        ref = region(u, ORDERS[colour], phase, place, rows)
        return pltpu.make_async_remote_copy(
            src_ref=ref,
            dst_ref=ref,
            send_sem=send_sem.at[u],
            recv_sem=recv_sem.at[u, stage, direction],
            device_id=peer,
            device_id_type=MESH,
        )

    def advance(colour, slot):
        for depth in (0, 5, 4, 3, 2, 1):
            chunk = slot - depth

            @pl.when((chunk >= 0) & (chunk * COLOURS + colour < UNITS))
            def _():
                if depth > 0:
                    for direction in range(2):
                        hop(colour, depth - 1, chunk, direction, True).wait_recv()
                if depth < STAGES:
                    for direction in range(2):
                        hop(colour, depth, chunk, direction, False).start()

    def row(ref):
        return ref[...].astype(F32).reshape(1, ref.shape[0])

    def rows_of(s):
        return pl.ds(pl.multiple_of(s * LENGTH, LENGTH), LENGTH)

    def squares():
        def one(s, _):
            part = x[rows_of(s), :].astype(F32)
            total = jnp.sum(part * part, axis=1, keepdims=True)
            sq[tp, rows_of(s), :] = jnp.broadcast_to(total, (LENGTH, LANES))
            return 0

        lax.fori_loop(0, SEQS, one, 0)

    def pool(s):
        total = sq[0, rows_of(s), :] + sq[1, rows_of(s), :]
        scale = lax.rsqrt(total / WIDTH + EPS)[:, :1]
        at = lax.broadcasted_iota(jnp.int32, (LENGTH, LENGTH), 0)
        col = lax.broadcasted_iota(jnp.int32, (LENGTH, LENGTH), 1)
        for g in range(2):
            reach = jnp.where(tp == 0, 1 << g, 4 << g)
            lower = jnp.maximum(at - reach, 0)
            upper = jnp.minimum(at + reach, LENGTH)
            band = jnp.where((col >= lower) & (col < upper), 1.0, 0.0).astype(BF16)
            count = (upper[:, :1] - lower[:, :1]).astype(F32)
            columns = slice(g * 512, (g + 1) * 512)
            piece = x[rows_of(s), columns].astype(F32) * scale * row(mix_gain)[:, columns]
            piece = piece.astype(BF16)
            window = jnp.dot(band, piece, preferred_element_type=F32)
            mixed[rows_of(s), columns] = (window / count - piece.astype(F32)).astype(BF16)

    def group(s):
        for g in range(2):
            columns = slice(g * 512, (g + 1) * 512)
            maps = w[U_POOL + g].reshape(32, 4, 16, LANES)
            right = jnp.concatenate([maps[:, ct].reshape(512, LANES) for ct in range(4)], axis=1)
            out = dot_nt(mixed[rows_of(s), columns], right) * pool_scale[g : g + 1, :]
            mixed[rows_of(s), columns] = out.astype(BF16)

    def project(side, block, dst):
        right = jnp.concatenate(
            [w[U_OUT + k, side, block].reshape(256, LANES) for k in range(8)], axis=1
        )
        columns = pl.ds(pl.multiple_of(block * 256, 256), 256)

        def one(s, _):
            dst[rows_of(s), columns] = dot_nt(mixed[rows_of(s), :], right).astype(BF16)
            return 0

        lax.fori_loop(0, SEQS, one, 0)

    def give_piece(block, index):
        columns = pl.ds(pl.multiple_of(block * 256, 256), 256)
        return across(give.at[:, columns], got.at[:, columns], index + block)

    def middle(s):
        total = own[rows_of(s), :].astype(F32) + got[rows_of(s), :].astype(F32)
        value = x[rows_of(s), :].astype(F32) + total * row(out_scale)
        mid[tp, rows_of(s), :] = value.astype(BF16)

    def mid_piece(s, side):
        ref = mid.at[side, rows_of(s), :]
        return across(ref, ref, 6 + s)

    def norm(s):
        left = mid[0, rows_of(s), :].astype(F32)
        right = mid[1, rows_of(s), :].astype(F32)
        total = jnp.sum(left * left + right * right, axis=1, keepdims=True)
        scale = lax.rsqrt(total / WIDTH + EPS)
        ours, theirs = row(gain), row(mate_gain)
        left_gain = jnp.where(tp == 0, ours, theirs)
        right_gain = jnp.where(tp == 0, theirs, ours)
        normed[rows_of(s), 0:HALF] = (left * scale * left_gain).astype(BF16)
        normed[rows_of(s), HALF:WIDTH] = (right * scale * right_gain).astype(BF16)

    def hidden_of(up_raw, gate_raw, columns):
        taps = conv_taps[:, columns]
        ups = up_scale[columns].reshape(1, -1)
        gates = gate_scale[columns].reshape(1, -1)
        lifted = (up_raw * ups).astype(BF16).astype(F32)
        at = lax.broadcasted_iota(jnp.int32, lifted.shape, 0)
        before = jnp.where(at == 0, 0.0, pltpu.roll(lifted, 1, 0))
        after = jnp.where(at == LENGTH - 1, 0.0, pltpu.roll(lifted, LENGTH - 1, 0))
        conv = taps[0:1] * before + taps[1:2] * lifted + taps[2:3] * after
        return (jax.nn.gelu(conv) * (gate_raw * gates)).astype(BF16)

    def pair(u):
        return jnp.concatenate(
            [w[u].reshape(WIDTH, LANES), w[u + 1].reshape(WIDTH, LANES)], axis=1
        )

    def feed(j, s):
        u = U_FF + 4 * j
        left = normed[rows_of(s), :]
        up_raw = jnp.dot(left, pair(u), preferred_element_type=F32)
        gate_raw = jnp.dot(left, pair(u + 2), preferred_element_type=F32)
        columns = pl.ds(pl.multiple_of(j * 256, 256), 256)
        hid[rows_of(s), columns] = hidden_of(up_raw, gate_raw, columns)

    def feed_last(s):
        both = jnp.dot(normed[rows_of(s), :], pair(U_LAST), preferred_element_type=F32)
        columns = pl.ds(10 * LANES, LANES)
        hid[rows_of(s), columns] = hidden_of(both[:, :LANES], both[:, LANES:], columns)

    def down_part(side, block, tiles):
        return jnp.concatenate(
            [w[U_DOWN + k, side, block].reshape(256, LANES) for k in tiles], axis=1
        )

    def down_first(s):
        def one(n, _):
            right = down_part(n // 4, lax.rem(n, 4), range(8))
            columns = pl.ds(pl.multiple_of(n * 256, 256), 256)
            acc[rows_of(s), columns] = dot_nt(hid[rows_of(s), 0:1024], right)
            return 0

        lax.fori_loop(0, 8, one, 0)

    def down_rest(side, block, dst):
        right = down_part(side, block, range(8, 11))
        wide = pl.ds(pl.multiple_of(side * HALF + block * 256, 256), 256)
        columns = pl.ds(pl.multiple_of(block * 256, 256), 256)

        def one(s, _):
            total = acc[rows_of(s), wide] + dot_nt(hid[rows_of(s), 1024:HID], right)
            dst[rows_of(s), columns] = total.astype(BF16)
            return 0

        lax.fori_loop(0, SEQS, one, 0)

    def compute(m):
        def during(start, count, body):
            @pl.when((m >= start) & (m < start + count))
            def _():
                body(m - start)

        def send_squares(_):
            squares()

        def start_squares(_):
            across(sq.at[tp], sq.at[tp], 1).start()

        def take_squares(_):
            across(sq.at[mate], sq.at[mate], 1).wait_recv()
            across(gain_hbm, mate_gain, 0).wait_recv()

        during(0, 1, send_squares)
        during(1, 1, start_squares)
        during(4, 1, take_squares)
        during(4, 4, pool)
        during(23, 4, group)

        def project_out(k):
            for part in range(2):
                project(mate, 2 * k + part, give)
                give_piece(2 * k + part, 2).start()

        def project_own(k):
            for part in range(2):
                project(tp, 2 * k + part, own)

        during(31, 2, project_out)
        during(33, 2, project_own)

        def take_mixer(_):
            for block in range(4):
                give_piece(block, 2).wait_recv()

        def middles(k):
            for part in range(2):
                middle(2 * k + part)
            for part in range(2):
                mid_piece(2 * k + part, tp).start()

        def norms(k):
            for part in range(2):
                mid_piece(2 * k + part, mate).wait_recv()
                norm(2 * k + part)

        during(35, 1, take_mixer)
        during(35, 2, middles)
        during(37, 2, norms)
        during(39, 20, lambda k: feed(k // 4, lax.rem(k, 4)))
        during(59, 4, feed_last)
        during(59, 4, down_first)

    def micro(m, _):
        slot, turn = m // COLOURS, lax.rem(m, COLOURS)
        for colour in range(COLOURS):

            @pl.when(turn == colour)
            def _():
                advance(colour, slot)

        compute(m)
        return 0

    lax.fori_loop(0, SLOTS * COLOURS, micro, 0)

    for block in range(4):
        give_piece(block, 2).wait_send()
    for block in range(4):
        down_rest(mate, block, give)
        give_piece(block, 10).start()
    for block in range(4):
        down_rest(tp, block, own)
    for block in range(4):
        give_piece(block, 10).wait_recv()

    def finish(s, _):
        total = own[rows_of(s), :].astype(F32) + got[rows_of(s), :].astype(F32)
        value = mid[tp, rows_of(s), :].astype(F32) + total * row(down_scale)
        x[rows_of(s), :] = value.astype(BF16)
        return 0

    lax.fori_loop(0, SEQS, finish, 0)
    result = pltpu.make_async_copy(x, y_hbm, y_sem)
    result.start()

    across(gain_hbm, mate_gain, 0).wait_send()
    across(sq.at[tp], sq.at[tp], 1).wait_send()
    for s in range(SEQS):
        mid_piece(s, tp).wait_send()
    for block in range(4):
        give_piece(block, 10).wait_send()

    def drain(u, _):
        same_size = normed.at[pl.ds(0, 31 * 32), pl.ds(0, 256)]
        pltpu.make_async_copy(same_size, same_size, send_sem.at[u]).wait()
        return 0

    lax.fori_loop(0, UNITS, drain, 0)
    result.wait()


def layer(
    layer_in,
    mix_gain,
    pool_weight,
    pool_scale,
    out_weight,
    out_scale,
    channel_gain,
    up_weight,
    up_scale,
    gate_weight,
    gate_scale,
    conv_weight,
    down_weight,
    down_scale,
):
    anywhere = pl.BlockSpec(memory_space=pl.ANY)
    dma = pltpu.SemaphoreType.DMA
    return pl.pallas_call(
        kernel,
        out_shape=jax.ShapeDtypeStruct((ROWS, HALF), BF16),
        in_specs=[anywhere] * 14,
        out_specs=anywhere,
        scratch_shapes=[
            pltpu.VMEM((UNITS, 2, 4, 4, 64, LANES), BF16),
            pltpu.VMEM((ROWS, HALF), BF16),
            pltpu.VMEM((ROWS, HALF), BF16),
            pltpu.VMEM((ROWS, HALF), BF16),
            pltpu.VMEM((ROWS, HALF), BF16),
            pltpu.VMEM((ROWS, HALF), BF16),
            pltpu.VMEM((2, ROWS, HALF), BF16),
            pltpu.VMEM((ROWS, WIDTH), BF16),
            pltpu.VMEM((ROWS, HID), BF16),
            pltpu.VMEM((ROWS, WIDTH), F32),
            pltpu.VMEM((2, 16, 512), F32),
            pltpu.VMEM((64, HALF), F32),
            pltpu.VMEM((64, HID), F32),
            pltpu.VMEM((64, HID), F32),
            pltpu.VMEM((64, HID), F32),
            pltpu.VMEM((HALF,), BF16),
            pltpu.VMEM((2, 512), F32),
            pltpu.VMEM((HALF,), F32),
            pltpu.VMEM((HALF,), BF16),
            pltpu.VMEM((HALF,), BF16),
            pltpu.VMEM((HID,), F32),
            pltpu.VMEM((HID,), F32),
            pltpu.VMEM((3, HID), F32),
            pltpu.VMEM((HALF,), F32),
            pltpu.VMEM((2, ROWS, LANES), F32),
            dma((14,)),
            dma((UNITS,)),
            dma((UNITS, STAGES, 2)),
            dma((14,)),
            dma((14,)),
            dma,
        ],
        compiler_params=pltpu.CompilerParams(
            collective_id=0, has_side_effects=True, vmem_limit_bytes=66_000_000
        ),
    )(
        layer_in,
        pool_weight.transpose(0, 2, 1),
        out_weight.T,
        up_weight,
        gate_weight,
        down_weight.T,
        mix_gain,
        pool_scale,
        out_scale,
        channel_gain,
        up_scale,
        gate_scale,
        conv_weight,
        down_scale,
    )


def solution(mesh):
    torus = Mesh(
        mesh.devices.reshape(mesh.shape["rep"], 2, 4, 4, mesh.shape["tp"]),
        ("rep", "fs_0", "fs_1", "fs_2", "tp"),
    )
    in_specs = (
        P(REP_FS, "tp"),
        P("tp"),
        P("tp", None, FS),
        P("tp", None),
        P("tp", FS),
        P("tp"),
        P("tp"),
        P(FS, "tp"),
        P("tp"),
        P(FS, "tp"),
        P("tp"),
        P(None, "tp"),
        P("tp", FS),
        P("tp"),
    )
    out_specs = P(REP_FS, "tp")
    return jax.shard_map(
        layer, mesh=torus, in_specs=in_specs, out_specs=out_specs, check_vma=False
    )
```

```python
import functools

import jax
import jax.numpy as jnp
from jax import lax
from jax.experimental import pallas as pl
from jax.experimental.pallas import tpu as pltpu
from jax.sharding import Mesh
from jax.sharding import PartitionSpec as P

LENGTH = 256
FS = ("fs_0", "fs_1", "fs_2")
REP_FS = ("rep", "fs_0", "fs_1", "fs_2")
EPS = 1e-06

F32 = jnp.float32
BF16 = jnp.bfloat16
MESH = pl.DeviceIdType.MESH

ROWS = 1024
HALF = 1024
WIDTH = 2048
HID = 1408
SEQS = ROWS // LENGTH
LANES = 128

U_POOL = 0
U_OUT = 2
U_LAST = 10
U_FF = 12
U_DOWN = 32
UNITS = 43
STAGES = 5

ORDERS = (
    "xyz",
    "xyz",
    "xyz",
    "yzx",
    "yzx",
    "xyz",
    "xzy",
    "xyz",
    "yzx",
    "xyz",
    "xzy",
    "yxz",
    "xyz",
    "xyz",
    "xyz",
    "xzy",
    "xzy",
    "yxz",
    "yzx",
    "yxz",
    "zxy",
    "yzx",
    "xyz",
    "yxz",
    "yzx",
    "xzy",
    "yxz",
    "yzx",
    "xyz",
    "yxz",
    "yxz",
    "zxy",
    "yzx",
    "yxz",
    "yxz",
    "zxy",
    "xyz",
    "zxy",
    "yxz",
    "yzx",
    "yzx",
    "zxy",
    "yxz",
)

SCHEDULE = (
    (48, 120, 80, 128, 200, 168, 64, 24, 32, 192, 296, 160, 248, 328, 280,),
    (72, 8, 104, 16, 0, 144, 320, 216, 312, 256,),
    (
        40, 152, 56, 232, 96, 1048, 136, 49, 1168, 112, 1296, 1120, 169, 1160, 184, 1064, 121, 1248,
        1080, 81, 1328, 65, 1024, 297, 1280, 1128, 25, 88, 1032, 1200,
    ),
    (1192, 1072, 1144, 1008, 73, 9, 129, 201, 161, 33, 193, 145, 208, 264,),
    (1320, 1104, 1216, 1016, 1312, 1000, 1256, 105, 17, 1, 249, 321, 217, 313, 240, 257, 272,),
    (
        1040, 1152, 1056, 1232, 1096, 1049, 1136, 1169, 1112, 41, 57, 97, 113, 153, 233, 137, 304,
        336, 50, 170,
    ),
    (
        1121, 1184, 1081, 1065, 1025, 1088, 1297, 1033, 1073, 1193, 1009, 298, 329, 281, 74, 122,
        82, 1145, 1129, 1201, 130, 1208, 176, 10, 1264, 1321, 224, 1161, 202, 1217, 1105, 1313, 162,
        1017, 1001, 1240, 288, 66, 1257, 106, 1272, 1249, 250, 1153, 154, 1050, 1041, 26, 1233,
        1057, 1137, 1097, 1113, 1304, 1170, 34, 1298, 1336, 18, 171, 1122, 194, 1329, 1082, 146,
        1281, 1074, 75, 1176, 1130, 322, 1224, 185, 1162, 89, 1202, 2, 218, 1288, 1010, 1250, 177,
        1066, 314, 225, 67, 1026, 11, 258, 1106, 1154, 1034, 107, 1194, 42, 1018, 1146, 1075, 76,
        155, 1185, 1089, 1322, 19, 234, 1171, 1218, 1177, 58, 1225, 1002, 1314, 172, 1011, 12, 1258,
        3, 1107, 209, 265, 27, 98, 1067, 108, 1042, 1155, 43, 1019, 1076, 241, 273, 51, 1234, 235,
        1058, 20, 68, 1003, 1209, 1172, 1265, 1012, 35, 59, 1098, 99, 4, 1043, 1241, 1273, 114,
        1027, 1108, 1235, 28, 305, 178, 1068, 44, 195, 1051, 52, 1059, 1020, 1099, 299, 1035, 60,
        36, 1114, 1305, 1004,
    ),
    (1028, 1178, 138, 115,),
    (330, 179, 100, 289, 1052, 186, 123, 1044, 1195, 196, 1036, 156, 1299, 147, 300, 1060, 1115,),
    (1138, 1330, 1289, 1179, 337, 83,),
    (116,),
    (1186, 1100, 139, 187,),
    (1196, 1123, 90, 124,),
    (1300, 180,),
    (1337, 1156, 210, 131,),
    (1147, 148,),
    (1139, 1187, 266, 236,),
    (1083, 84,),
    (1116,),
    (1090,),
    (1124, 91, 226, 323, 140, 1210, 163,),
    (1180,),
    (1148,),
    (1131,),
    (211, 188,),
    (1266, 1084, 1091, 1236, 267, 242, 132,),
    (1226, 219, 227, 203, 92,),
    (),
    (1323, 1140, 1211, 1163, 1267, 324, 212, 164, 1132,),
    (1242, 1188, 1227, 243, 290,),
    (274, 251, 228,),
    (1219, 1092, 220,),
    (1203, 1324, 282, 306, 268, 1164,),
    (1243, 315, 204,),
    (1212, 1290, 1274, 291, 331,),
    (1220, 244,),
    (1282, 1228, 1251, 275, 338, 1306, 252, 1204,),
    (1291, 307, 259, 283, 292,),
    (1268, 1315,),
    (1275, 276,),
    (1331, 1244, 1338, 339, 316, 332,),
    (1252, 1307, 308,),
    (1292,),
    (1283, 1259, 260, 284,),
    (1339, 1332, 340,),
    (1276, 1316,),
    (1260, 1284, 1308,),
    (),
    (),
    (1340,),
    (),
    (),
    (),
    (),
    (),
)

PIECES = (
    ("squares", 1),
    ("share", 1),
    ("pool", 4),
    ("group", 2),
    ("project", 8),
    ("middle", 4),
    ("norm", 4),
    ("feed", 20),
    ("last", 2),
    ("down", 8),
)
TOTAL = sum(count for _, count in PIECES)


def steps_of(order):
    steps = []
    for phase, dim in enumerate(order):
        steps += [(phase, "a")] if dim == "z" else [(phase, "a"), (phase, "b")]
    return steps


AXIS = {"x": "fs_2", "y": "fs_1"}


def dot_nt(left, right):
    return lax.dot_general(left, right, (((1,), (1,)), ((), ())), preferred_element_type=F32)


def kernel(
    x_hbm,
    pool_hbm,
    out_hbm,
    up_hbm,
    gate_hbm,
    down_hbm,
    mix_gain_hbm,
    pool_scale_hbm,
    out_scale_hbm,
    gain_hbm,
    up_scale_hbm,
    gate_scale_hbm,
    conv_hbm,
    down_scale_hbm,
    y_hbm,
    w,
    x,
    mixed,
    give,
    got,
    own,
    mid,
    normed,
    hid,
    acc,
    raw,
    st_pool,
    st_out,
    st_up,
    st_gate,
    st_down,
    mix_gain,
    pool_scale,
    out_scale,
    gain,
    mate_gain,
    up_scale,
    gate_scale,
    conv_taps,
    down_scale,
    sq,
    in_sem,
    send_sem,
    recv_sem,
    tp_send,
    tp_recv,
    y_sem,
):
    rep = lax.axis_index("rep")
    zl = lax.axis_index("fs_0")
    me = {"z": zl, "y": lax.axis_index("fs_1"), "x": lax.axis_index("fs_2")}
    tp = lax.axis_index("tp")
    mate = 1 - tp
    zz = rep * 2 + zl
    z_up = lax.rem(zz + 1, 4)
    z_down = lax.rem(zz + 3, 4)

    def to_z(place):
        return {"rep": place // 2, "fs_0": lax.rem(place, 2)}

    def ring(dim, shift):
        return lax.rem(me[dim] + shift + 4, 4)

    peers = [to_z(z_up), to_z(z_down), {"tp": mate}]
    for dim in ("x", "y"):
        peers += [{AXIS[dim]: ring(dim, 1)}, {AXIS[dim]: ring(dim, -1)}]

    loads = [
        pltpu.make_async_copy(src, dst, in_sem.at[k])
        for k, (src, dst) in enumerate(
            (
                (pool_hbm, st_pool),
                (out_hbm, st_out),
                (up_hbm, st_up),
                (gate_hbm, st_gate),
                (down_hbm, st_down),
                (x_hbm, x),
                (mix_gain_hbm, mix_gain),
                (pool_scale_hbm, pool_scale),
                (out_scale_hbm, out_scale),
                (gain_hbm, gain),
                (up_scale_hbm, up_scale),
                (gate_scale_hbm, gate_scale),
                (conv_hbm, conv_taps),
                (down_scale_hbm, down_scale),
            )
        )
    ]
    for load in loads:
        load.start()

    barrier = pltpu.get_barrier_semaphore()
    for peer in peers:
        pl.semaphore_signal(barrier, inc=1, device_id=peer, device_id_type=MESH)

    for load in loads:
        load.wait()

    mine = (me["z"], me["y"], me["x"])
    for g in range(2):
        for ct in range(4):
            block = st_pool[g, :, ct * LANES : (ct + 1) * LANES]
            w[(U_POOL + g, *mine, pl.ds(ct * 16, 16), slice(None))] = block.astype(BF16)
    for k in range(8):
        w[(U_OUT + k, *mine)] = st_out[:, k * LANES : (k + 1) * LANES].astype(BF16)
    for k in range(11):
        w[(U_DOWN + k, *mine)] = st_down[:, k * LANES : (k + 1) * LANES].astype(BF16)
        columns = slice(k * LANES, (k + 1) * LANES)
        at_up = U_LAST if k == 10 else U_FF + 4 * (k // 2) + k % 2
        at_gate = U_LAST + 1 if k == 10 else U_FF + 4 * (k // 2) + 2 + k % 2
        w[(at_up, *mine)] = st_up[:, columns].astype(BF16)
        w[(at_gate, *mine)] = st_gate[:, columns].astype(BF16)

    pl.semaphore_wait(barrier, len(peers))

    def across(src, dst, index):
        return pltpu.make_async_remote_copy(
            src_ref=src,
            dst_ref=dst,
            send_sem=tp_send.at[index],
            recv_sem=tp_recv.at[index],
            device_id={"tp": mate},
            device_id_type=MESH,
        )

    across(gain_hbm, mate_gain, 0).start()

    def region(u, order, phase, place, rows):
        picks = {}
        for k, dim in enumerate(order):
            if k < phase:
                picks[dim] = slice(None)
            elif k == phase:
                picks[dim] = pl.ds(place, 1)
            else:
                picks[dim] = pl.ds(me[dim], 1)
        return w.at[u, picks["z"], picks["y"], picks["x"], rows, :]

    every, first, second = pl.ds(0, 64), pl.ds(0, 32), pl.ds(32, 32)

    def moves(u, stage):
        order = ORDERS[u]
        phase, step = steps_of(order)[stage]
        dim = order[phase]
        if dim == "z":
            there = 1 - zl
            return phase, (
                (zl, first, to_z(z_up), there, first),
                (zl, second, to_z(z_down), there, second),
            )
        right, left = {AXIS[dim]: ring(dim, 1)}, {AXIS[dim]: ring(dim, -1)}
        if step == "a":
            return phase, (
                (me[dim], every, right, ring(dim, -1), every),
                (me[dim], every, left, ring(dim, 1), every),
            )
        return phase, (
            (ring(dim, -1), first, right, ring(dim, 2), first),
            (ring(dim, 1), second, left, ring(dim, 2), second),
        )

    def hop(u, stage, direction, arriving):
        phase, both = moves(u, stage)
        place, rows, peer, from_place, from_rows = both[direction]
        if arriving:
            place, rows = from_place, from_rows
        ref = region(u, ORDERS[u], phase, place, rows)
        return pltpu.make_async_remote_copy(
            src_ref=ref,
            dst_ref=ref,
            send_sem=send_sem.at[u],
            recv_sem=recv_sem.at[u, stage, direction],
            device_id=peer,
            device_id_type=MESH,
        )

    def gather(position):
        for code in SCHEDULE[position]:
            arriving, (u, stage) = code >= 1000, divmod(code % 1000, 8)
            for direction in range(2):
                copy = hop(u, stage, direction, arriving)
                if arriving:
                    copy.wait_recv()
                else:
                    copy.start()

    def row(ref):
        return ref[...].astype(F32).reshape(1, ref.shape[0])

    def rows_of(s):
        return pl.ds(pl.multiple_of(s * LENGTH, LENGTH), LENGTH)

    def squares():
        def one(s, _):
            part = x[rows_of(s), :].astype(F32)
            total = jnp.sum(part * part, axis=1, keepdims=True)
            sq[tp, rows_of(s), :] = jnp.broadcast_to(total, (LENGTH, LANES))
            return 0

        lax.fori_loop(0, SEQS, one, 0)

    def pool(s):
        total = sq[0, rows_of(s), :] + sq[1, rows_of(s), :]
        scale = lax.rsqrt(total / WIDTH + EPS)[:, :1]
        at = lax.broadcasted_iota(jnp.int32, (LENGTH, LENGTH), 0)
        col = lax.broadcasted_iota(jnp.int32, (LENGTH, LENGTH), 1)
        for g in range(2):
            reach = jnp.where(tp == 0, 1 << g, 4 << g)
            lower = jnp.maximum(at - reach, 0)
            upper = jnp.minimum(at + reach, LENGTH)
            band = jnp.where((col >= lower) & (col < upper), 1.0, 0.0).astype(BF16)
            count = (upper[:, :1] - lower[:, :1]).astype(F32)
            columns = slice(g * 512, (g + 1) * 512)
            piece = x[rows_of(s), columns].astype(F32) * scale * row(mix_gain)[:, columns]
            piece = piece.astype(BF16)
            window = jnp.dot(band, piece, preferred_element_type=F32)
            mixed[rows_of(s), columns] = (window / count - piece.astype(F32)).astype(BF16)

    def group(g):
        columns = pl.ds(pl.multiple_of(g * 512, 512), 512)
        maps = w[U_POOL + g].reshape(32, 4, 16, LANES)
        right = jnp.concatenate([maps[:, ct].reshape(512, LANES) for ct in range(4)], axis=1)
        out = dot_nt(mixed[:, columns], right) * pool_scale[pl.ds(g, 1), :]
        normed[:, columns] = out.astype(BF16)

    def project(side, block, dst):
        right = jnp.concatenate(
            [w[U_OUT + k, side, block].reshape(256, LANES) for k in range(8)], axis=1
        )
        columns = pl.ds(pl.multiple_of(block * 256, 256), 256)
        dst[:, columns] = dot_nt(normed[:, 0:HALF], right).astype(BF16)

    def give_piece(block, index):
        columns = pl.ds(pl.multiple_of(block * 256, 256), 256)
        return across(give.at[:, columns], got.at[:, columns], index + block)

    def middle(s):
        total = own[rows_of(s), :].astype(F32) + got[rows_of(s), :].astype(F32)
        value = x[rows_of(s), :].astype(F32) + total * row(out_scale)
        mid[tp, rows_of(s), :] = value.astype(BF16)

    def mid_piece(s, side):
        ref = mid.at[side, rows_of(s), :]
        return across(ref, ref, 6 + s)

    def norm(s):
        left = mid[0, rows_of(s), :].astype(F32)
        right = mid[1, rows_of(s), :].astype(F32)
        total = jnp.sum(left * left + right * right, axis=1, keepdims=True)
        scale = lax.rsqrt(total / WIDTH + EPS)
        ours, theirs = row(gain), row(mate_gain)
        left_gain = jnp.where(tp == 0, ours, theirs)
        right_gain = jnp.where(tp == 0, theirs, ours)
        normed[rows_of(s), 0:HALF] = (left * scale * left_gain).astype(BF16)
        normed[rows_of(s), HALF:WIDTH] = (right * scale * right_gain).astype(BF16)

    def hidden_of(up_raw, gate_raw, columns):
        taps = conv_taps[:, columns]
        ups = up_scale[columns].reshape(1, -1)
        gates = gate_scale[columns].reshape(1, -1)
        lifted = (up_raw * ups).astype(BF16).astype(F32)
        at = lax.broadcasted_iota(jnp.int32, lifted.shape, 0)
        before = jnp.where(at == 0, 0.0, pltpu.roll(lifted, 1, 0))
        after = jnp.where(at == LENGTH - 1, 0.0, pltpu.roll(lifted, LENGTH - 1, 0))
        conv = taps[0:1] * before + taps[1:2] * lifted + taps[2:3] * after
        return (jax.nn.gelu(conv) * (gate_raw * gates)).astype(BF16)

    def pair(u):
        return jnp.concatenate(
            [w[u].reshape(WIDTH, LANES), w[u + 1].reshape(WIDTH, LANES)], axis=1
        )

    def half_of(h):
        return pl.ds(pl.multiple_of(h * 512, 512), 512)

    def feed_up(j, h):
        left = normed[half_of(h), :]
        raw[...] = jnp.dot(left, pair(U_FF + 4 * j), preferred_element_type=F32)

    def feed_gate(j, h):
        left = normed[half_of(h), :]
        gate_raw = jnp.dot(left, pair(U_FF + 4 * j + 2), preferred_element_type=F32)
        columns = pl.ds(pl.multiple_of(j * 256, 256), 256)
        for q in range(2):
            part = slice(q * LENGTH, (q + 1) * LENGTH)
            hid[rows_of(2 * h + q), columns] = hidden_of(raw[part, :], gate_raw[part], columns)

    def feed_last(h):
        both = jnp.dot(normed[half_of(h), :], pair(U_LAST), preferred_element_type=F32)
        columns = pl.ds(10 * LANES, LANES)
        for q in range(2):
            part = both[q * LENGTH : (q + 1) * LENGTH]
            hid[rows_of(2 * h + q), columns] = hidden_of(part[:, :LANES], part[:, LANES:], columns)

    def down_part(side, block, tiles):
        return jnp.concatenate(
            [w[U_DOWN + k, side, block].reshape(256, LANES) for k in tiles], axis=1
        )

    def down_first(n):
        right = down_part(n // 4, lax.rem(n, 4), range(8))
        columns = pl.ds(pl.multiple_of(n * 256, 256), 256)
        acc[:, columns] = dot_nt(hid[:, 0:1024], right)

    def down_rest(side, block, dst):
        right = down_part(side, block, range(8, 11))
        wide = pl.ds(pl.multiple_of(side * HALF + block * 256, 256), 256)
        columns = pl.ds(pl.multiple_of(block * 256, 256), 256)
        total = acc[:, wide] + dot_nt(hid[:, 1024:HID], right)
        dst[:, columns] = total.astype(BF16)

    def compute(m):
        start = 0
        starts = {}
        for name, count in PIECES:
            starts[name] = (start, count)
            start += count

        def during(name, body):
            first_one, count = starts[name]

            @pl.when((m >= first_one) & (m < first_one + count))
            def _():
                body(m - first_one)

        def share(_):
            across(sq.at[tp], sq.at[tp], 1).start()

        def pooling(s):
            @pl.when(s == 0)
            def _():
                across(sq.at[mate], sq.at[mate], 1).wait_recv()
                across(gain_hbm, mate_gain, 0).wait_recv()

            pool(s)

        def projecting(k):
            @pl.when(k < 4)
            def _():
                project(mate, k, give)
                give_piece(k, 2).start()

            @pl.when(k >= 4)
            def _():
                project(tp, k - 4, own)

        def middling(s):
            @pl.when(s == 0)
            def _():
                for block in range(4):
                    give_piece(block, 2).wait_recv()

            middle(s)
            mid_piece(s, tp).start()

        def norming(s):
            mid_piece(s, mate).wait_recv()
            norm(s)

        def feeding(k):
            j, h = k // 4, lax.rem(k, 4) // 2

            @pl.when(lax.rem(k, 2) == 0)
            def _():
                feed_up(j, h)

            @pl.when(lax.rem(k, 2) == 1)
            def _():
                feed_gate(j, h)

        during("squares", lambda _: squares())
        during("share", share)
        during("pool", pooling)
        during("group", group)
        during("project", projecting)
        during("middle", middling)
        during("norm", norming)
        during("feed", feeding)
        during("last", feed_last)
        during("down", down_first)

    def micro(m, _):
        def among(low, high):
            if high - low == 1:
                gather(low)
                return
            half = (low + high) // 2
            pl.when(m < half)(lambda: among(low, half))
            pl.when(m >= half)(lambda: among(half, high))

        among(0, TOTAL)
        compute(m)
        return 0

    lax.fori_loop(0, TOTAL, micro, 0)
    gather(TOTAL)

    for block in range(4):
        give_piece(block, 2).wait_send()

    def first_half(block, _):
        down_rest(mate, block, give)
        give_piece(block, 10).start()
        return 0

    lax.fori_loop(0, 4, first_half, 0)

    def result(block):
        columns = pl.ds(pl.multiple_of(block * 256, 256), 256)
        return pltpu.make_async_copy(x.at[:, columns], y_hbm.at[:, columns], y_sem.at[block])

    def second_half(block, _):
        columns = pl.ds(pl.multiple_of(block * 256, 256), 256)
        down_rest(tp, block, own)
        give_piece(block, 10).wait_recv()

        def finish(s, _):
            total = own[rows_of(s), columns].astype(F32) + got[rows_of(s), columns].astype(F32)
            scale = down_scale[columns].reshape(1, 256)
            value = mid[tp, rows_of(s), columns].astype(F32) + total * scale
            x[rows_of(s), columns] = value.astype(BF16)
            return 0

        lax.fori_loop(0, SEQS, finish, 0)
        result(block).start()
        return 0

    lax.fori_loop(0, 4, second_half, 0)

    across(gain_hbm, mate_gain, 0).wait_send()
    across(sq.at[tp], sq.at[tp], 1).wait_send()
    for s in range(SEQS):
        mid_piece(s, tp).wait_send()
    for block in range(4):
        give_piece(block, 10).wait_send()

    def drain(u, _):
        same_size = normed.at[pl.ds(0, 31 * 32), pl.ds(0, 256)]
        pltpu.make_async_copy(same_size, same_size, send_sem.at[u]).wait()
        return 0

    lax.fori_loop(0, UNITS, drain, 0)
    for block in range(4):
        result(block).wait()


def layer(
    layer_in,
    mix_gain,
    pool_weight,
    pool_scale,
    out_weight,
    out_scale,
    channel_gain,
    up_weight,
    up_scale,
    gate_weight,
    gate_scale,
    conv_weight,
    down_weight,
    down_scale,
):
    anywhere = pl.BlockSpec(memory_space=pl.ANY)
    dma = pltpu.SemaphoreType.DMA
    return pl.pallas_call(
        kernel,
        out_shape=jax.ShapeDtypeStruct((ROWS, HALF), BF16),
        in_specs=[anywhere] * 14,
        out_specs=anywhere,
        scratch_shapes=[
            pltpu.VMEM((UNITS, 2, 4, 4, 64, LANES), BF16),
            pltpu.VMEM((ROWS, HALF), BF16),
            pltpu.VMEM((ROWS, HALF), BF16),
            pltpu.VMEM((ROWS, HALF), BF16),
            pltpu.VMEM((ROWS, HALF), BF16),
            pltpu.VMEM((ROWS, HALF), BF16),
            pltpu.VMEM((2, ROWS, HALF), BF16),
            pltpu.VMEM((ROWS, WIDTH), BF16),
            pltpu.VMEM((ROWS, HID), BF16),
            pltpu.VMEM((ROWS, WIDTH), F32),
            pltpu.VMEM((512, 256), F32),
            pltpu.VMEM((2, 16, 512), F32),
            pltpu.VMEM((64, HALF), F32),
            pltpu.VMEM((64, HID), F32),
            pltpu.VMEM((64, HID), F32),
            pltpu.VMEM((64, HID), F32),
            pltpu.VMEM((HALF,), BF16),
            pltpu.VMEM((2, 512), F32),
            pltpu.VMEM((HALF,), F32),
            pltpu.VMEM((HALF,), BF16),
            pltpu.VMEM((HALF,), BF16),
            pltpu.VMEM((HID,), F32),
            pltpu.VMEM((HID,), F32),
            pltpu.VMEM((3, HID), F32),
            pltpu.VMEM((HALF,), F32),
            pltpu.VMEM((2, ROWS, LANES), F32),
            dma((14,)),
            dma((UNITS,)),
            dma((UNITS, STAGES, 2)),
            dma((14,)),
            dma((14,)),
            dma((4,)),
        ],
        compiler_params=pltpu.CompilerParams(
            collective_id=0, has_side_effects=True, vmem_limit_bytes=66_000_000
        ),
    )(
        layer_in,
        pool_weight.transpose(0, 2, 1),
        out_weight.T,
        up_weight,
        gate_weight,
        down_weight.T,
        mix_gain,
        pool_scale,
        out_scale,
        channel_gain,
        up_scale,
        gate_scale,
        conv_weight,
        down_scale,
    )


def solution(mesh):
    torus = Mesh(
        mesh.devices.reshape(mesh.shape["rep"], 2, 4, 4, mesh.shape["tp"]),
        ("rep", "fs_0", "fs_1", "fs_2", "tp"),
    )
    in_specs = (
        P(REP_FS, "tp"),
        P("tp"),
        P("tp", None, FS),
        P("tp", None),
        P("tp", FS),
        P("tp"),
        P("tp"),
        P(FS, "tp"),
        P("tp"),
        P(FS, "tp"),
        P("tp"),
        P(None, "tp"),
        P("tp", FS),
        P("tp"),
    )
    out_specs = P(REP_FS, "tp")
    return jax.shard_map(
        layer, mesh=torus, in_specs=in_specs, out_specs=out_specs, check_vma=False
    )
```

```python
import jax
import jax.numpy as jnp
from jax import lax
from jax.experimental import pallas as pl
from jax.experimental.pallas import tpu as pltpu
from jax.sharding import Mesh
from jax.sharding import PartitionSpec as P

LENGTH = 256
FS = ("fs_0", "fs_1", "fs_2")
REP_FS = ("rep", "fs_0", "fs_1", "fs_2")
EPS = 1e-06

F32 = jnp.float32
BF16 = jnp.bfloat16
MESH = pl.DeviceIdType.MESH

ROWS = 1024
HALF = 1024
WIDTH = 2048
HID = 1408
SEQS = ROWS // LENGTH
LANES = 128
PAIR = 2 * LANES

U_POOL = 0
U_OUT = 1
U_LAST = 5
U_FF = 6
U_DOWN = 16
U_END = 21
UNITS = 22
STAGES = 5
SEND_GROUP = 3
FIRST_K = 4

ORDERS = (
    "xyz",
    "yzx",
    "xyz",
    "xyz",
    "xyz",
    "yzx",
    "yzx",
    "xyz",
    "xyz",
    "xzy",
    "yzx",
    "yxz",
    "xyz",
    "yzx",
    "xzy",
    "xzy",
    "yxz",
    "yzx",
    "zxy",
    "xyz",
    "yxz",
    "zxy",
)

SCHEDULE = (
    (24, 72, 8, 104, 144, 168,),
    (0, 48, 32, 80, 112, 40, 16, 136, 64, 88, 1144, 1168, 1024, 1008, 25, 9, 120, 128, 1072, 1104,),
    (1000, 1048, 1, 56, 105, 49, 160,),
    (1032, 1080, 1112, 1040, 33, 96, 81, 41,),
    (1016, 1136, 17, 145, 137,),
    (
        1064, 1088, 1025, 1009, 26, 10, 65, 1120, 1128, 73, 1001, 1105, 106, 152, 1049, 1056, 57,
        1033, 1160, 2, 50, 113, 1081, 169, 1096, 1041, 1017, 1137, 97, 121, 82, 1145, 146, 1065,
        1010, 11, 34, 42, 1073, 1152, 1026, 1057, 1106, 74, 1113, 1169, 1097, 1050, 27, 114, 1121,
        1146, 1002, 1082, 3, 122, 107, 1042, 89, 138, 129, 18, 1034, 1074, 1027, 28, 1114, 35, 1011,
        1003, 1122, 1089, 1129, 66, 12, 1138, 4, 1018, 19, 90, 1035, 75, 1107, 108, 1028, 1066,
        1012, 36, 1019, 130, 67, 1090, 161, 58, 153, 1004,
    ),
    (1108, 51,),
    (20, 1075, 76, 1067, 1161, 1130, 1153, 98, 1036, 162, 1058, 68, 59, 83, 1076, 154, 1051, 1020,),
    (1098,),
    (1162, 99,),
    (1059, 115, 60,),
    (52,),
    (),
    (1154,),
    (1068, 91,),
    (1099, 1083, 84, 100, 155, 123, 1052, 131,),
    (1091,),
    (1060, 43,),
    (1115, 92,),
    (1155, 1084,),
    (1131, 116,),
    (1100, 139,),
    (147, 132,),
    (1123,),
    (1043, 1116, 44, 1092,),
    (124, 156,),
    (170, 163,),
    (1139, 1147, 140, 148,),
    (1132, 1044, 1170, 171, 1124,),
    (1163, 164,),
    (1148, 1156, 1140,),
    (),
    (),
    (1171, 172,),
    (),
    (),
    (),
    (),
    (1164, 1172,),
)

PIECES = (
    ("share", 1),
    ("pool", 4),
    ("group", 2),
    ("project", 8),
    ("norm", 4),
    ("feed", 10),
    ("last", 1),
    ("down", 8),
)
TOTAL = sum(count for _, count in PIECES)

AXIS = {"x": "fs_2", "y": "fs_1"}

X_GAIN, X_SCALE, X_INPUT, X_MIXER, X_FINAL = 0, 1, 2, 3, 11


def steps_of(order):
    steps = []
    for phase, dim in enumerate(order):
        steps += [(phase, "a")] if dim == "z" else [(phase, "a"), (phase, "b")]
    return steps


def shards_in(order, stage):
    phase, step = steps_of(order)[stage]
    held = 1
    for dim in order[:phase]:
        held *= 2 if dim == "z" else 4
    return held if order[phase] == "z" or step == "b" else 2 * held


def dot_nt(left, right):
    return lax.dot_general(left, right, (((1,), (1,)), ((), ())), preferred_element_type=F32)


def kernel(
    x_hbm,
    pool_hbm,
    out_hbm,
    up_hbm,
    gate_hbm,
    down_hbm,
    mix_gain_hbm,
    pool_scale_hbm,
    out_scale_hbm,
    gain_hbm,
    up_scale_hbm,
    gate_scale_hbm,
    conv_hbm,
    down_scale_hbm,
    y,
    w,
    w_end,
    x,
    part,
    got,
    end,
    mid,
    normed,
    hid,
    acc,
    raw,
    st_pool,
    st_out,
    st_up,
    st_gate,
    st_down,
    mix_gain,
    pool_scale,
    out_scale,
    mate_out_scale,
    gain,
    mate_gain,
    up_scale,
    gate_scale,
    conv_taps,
    down_scale,
    in_sem,
    send_sem,
    recv_sem,
    tp_send,
    tp_recv,
    y_sem,
):
    rep = lax.axis_index("rep")
    zl = lax.axis_index("fs_0")
    me = {"z": zl, "y": lax.axis_index("fs_1"), "x": lax.axis_index("fs_2")}
    tp = lax.axis_index("tp")
    mate = 1 - tp
    zz = rep * 2 + zl
    z_up = lax.rem(zz + 1, 4)
    z_down = lax.rem(zz + 3, 4)

    def to_z(place):
        return {"rep": place // 2, "fs_0": lax.rem(place, 2)}

    def ring(dim, shift):
        return lax.rem(me[dim] + shift + 4, 4)

    peers = [to_z(z_up), to_z(z_down), {"tp": mate}]
    for dim in ("x", "y"):
        peers += [{AXIS[dim]: ring(dim, 1)}, {AXIS[dim]: ring(dim, -1)}]

    barrier = pltpu.get_barrier_semaphore()
    for peer in peers:
        pl.semaphore_signal(barrier, inc=1, device_id=peer, device_id_type=MESH)

    loads = [
        pltpu.make_async_copy(src, dst, in_sem.at[k])
        for k, (src, dst) in enumerate(
            (
                (pool_hbm, st_pool),
                (out_hbm, st_out),
                (up_hbm, st_up),
                (gate_hbm, st_gate),
                (down_hbm, st_down),
                (x_hbm, x.at[tp]),
                (mix_gain_hbm, mix_gain),
                (pool_scale_hbm, pool_scale),
                (out_scale_hbm, out_scale),
                (gain_hbm, gain),
                (up_scale_hbm, up_scale),
                (gate_scale_hbm, gate_scale),
                (conv_hbm, conv_taps),
                (down_scale_hbm, down_scale),
            )
        )
    ]
    for load in loads:
        load.start()
    for load in loads[:5]:
        load.wait()

    mine = (me["z"], me["y"], me["x"])
    for g in range(2):
        for ct in range(4):
            block = st_pool[g, :, ct * LANES : (ct + 1) * LANES]
            lanes = pl.ds(g * LANES, LANES)
            w[(U_POOL, *mine, pl.ds(ct * 16, 16), lanes)] = block.astype(BF16)
    for k in range(4):
        w[(U_OUT + k, *mine)] = st_out[:, k * PAIR : (k + 1) * PAIR].astype(BF16)
    for k in range(5):
        columns = slice(k * PAIR, (k + 1) * PAIR)
        w[(U_DOWN + k, *mine)] = st_down[:, columns].astype(BF16)
        w[(U_FF + 2 * k, *mine)] = st_up[:, columns].astype(BF16)
        w[(U_FF + 2 * k + 1, *mine)] = st_gate[:, columns].astype(BF16)
    rest = slice(10 * LANES, HID)
    w[(U_LAST, *mine, slice(None), pl.ds(0, LANES))] = st_up[:, rest].astype(BF16)
    w[(U_LAST, *mine, slice(None), pl.ds(LANES, LANES))] = st_gate[:, rest].astype(BF16)
    w_end[mine] = st_down[:, rest].astype(BF16)

    pl.semaphore_wait(barrier, len(peers))

    def across(src, dst, index):
        return pltpu.make_async_remote_copy(
            src_ref=src,
            dst_ref=dst,
            send_sem=tp_send.at[index],
            recv_sem=tp_recv.at[index],
            device_id={"tp": mate},
            device_id_type=MESH,
        )

    def region(u, order, phase, place, rows):
        picks = {}
        for k, dim in enumerate(order):
            if k < phase:
                picks[dim] = slice(None)
            elif k == phase:
                picks[dim] = pl.ds(place, 1)
            else:
                picks[dim] = pl.ds(me[dim], 1)
        where = (picks["z"], picks["y"], picks["x"], rows, slice(None))
        return w_end.at[where] if u == U_END else w.at[(u, *where)]

    every, first, second = pl.ds(0, 64), pl.ds(0, 32), pl.ds(32, 32)

    def moves(u, stage):
        order = ORDERS[u]
        phase, step = steps_of(order)[stage]
        dim = order[phase]
        if dim == "z":
            return phase, ((zl, first, to_z(z_up)), (zl, second, to_z(z_down)))
        right, left = {AXIS[dim]: ring(dim, 1)}, {AXIS[dim]: ring(dim, -1)}
        if step == "a":
            return phase, ((me[dim], every, right), (me[dim], every, left))
        return phase, ((ring(dim, -1), first, right), (ring(dim, 1), second, left))

    def send(u, stage):
        phase, both = moves(u, stage)
        for place, rows, peer in both:
            ref = region(u, ORDERS[u], phase, place, rows)
            pltpu.make_async_remote_copy(
                src_ref=ref,
                dst_ref=ref,
                send_sem=send_sem.at[u // SEND_GROUP],
                recv_sem=recv_sem.at[u, stage],
                device_id=peer,
                device_id_type=MESH,
            ).start()

    def arrived(u, stage):
        count = shards_in(ORDERS[u], stage)
        box = {1: (1, 1, 1), 2: (1, 1, 2), 4: (1, 1, 4), 8: (1, 2, 4), 16: (1, 4, 4)}[count]
        where = tuple(pl.ds(0, size) for size in box)
        ref = w_end.at[where] if u == U_END else w.at[(u, *where)]
        pltpu.make_async_copy(ref, ref, recv_sem.at[u, stage]).wait()

    def gather(position):
        for code in SCHEDULE[position]:
            u, stage = divmod(code % 1000, 8)
            (arrived if code >= 1000 else send)(u, stage)

    def row(ref):
        return ref[...].astype(F32).reshape(1, ref.shape[0])

    def rows_of(s):
        return pl.ds(pl.multiple_of(s * LENGTH, LENGTH), LENGTH)

    def block_of(n):
        return pl.ds(pl.multiple_of(n * PAIR, PAIR), PAIR)

    mixed = hid

    def pool(s):
        total = jnp.zeros((LENGTH, 1), F32)
        for side in range(2):
            values = x[side, rows_of(s), :].astype(F32)
            total = total + jnp.sum(values * values, axis=1, keepdims=True)
        scale = lax.rsqrt(total / WIDTH + EPS)
        at = lax.broadcasted_iota(jnp.int32, (LENGTH, LENGTH), 0)
        col = lax.broadcasted_iota(jnp.int32, (LENGTH, LENGTH), 1)
        for g in range(2):
            reach = jnp.where(tp == 0, 1 << g, 4 << g)
            lower = jnp.maximum(at - reach, 0)
            upper = jnp.minimum(at + reach, LENGTH)
            band = jnp.where((col >= lower) & (col < upper), 1.0, 0.0).astype(BF16)
            count = (upper[:, :1] - lower[:, :1]).astype(F32)
            columns = slice(g * 512, (g + 1) * 512)
            piece = x[tp, rows_of(s), columns].astype(F32) * scale * row(mix_gain)[:, columns]
            piece = piece.astype(BF16)
            window = jnp.dot(band, piece, preferred_element_type=F32)
            mixed[rows_of(s), columns] = (window / count - piece.astype(F32)).astype(BF16)

    def group(g):
        columns = pl.ds(pl.multiple_of(g * 512, 512), 512)
        lanes = pl.ds(pl.multiple_of(g * LANES, LANES), LANES)
        maps = w[U_POOL, :, :, :, :, lanes].reshape(32, 4, 16, LANES)
        right = jnp.concatenate([maps[:, ct].reshape(512, LANES) for ct in range(4)], axis=1)
        out = dot_nt(mixed[:, columns], right) * pool_scale[pl.ds(g, 1), :]
        normed[:, columns] = out.astype(BF16)

    def project(side, block):
        right = jnp.concatenate(
            [w[U_OUT + k, side, block].reshape(256, PAIR) for k in range(4)], axis=1
        )
        part[side, :, block_of(block)] = dot_nt(normed[:, 0:HALF], right).astype(BF16)

    def mixer_piece(side, block):
        columns = block_of(block)
        index = X_MIXER + side * 4 + block
        return across(part.at[side, :, columns], got.at[side, :, columns], index)

    def final_piece(block):
        columns = block_of(block)
        return across(part.at[mate, :, columns], end.at[:, columns], X_FINAL + block)

    def norm(s):
        ours, theirs = row(gain), row(mate_gain)
        gains = (jnp.where(tp == 0, ours, theirs), jnp.where(tp == 0, theirs, ours))
        ours, theirs = row(out_scale), row(mate_out_scale)
        scales = (jnp.where(tp == 0, ours, theirs), jnp.where(tp == 0, theirs, ours))
        total = jnp.zeros((LENGTH, 1), F32)
        for side in range(2):
            added = part[side, rows_of(s), :].astype(F32) + got[side, rows_of(s), :].astype(F32)
            value = x[side, rows_of(s), :].astype(F32) + added * scales[side]
            value = value.astype(BF16)
            mid[side, rows_of(s), :] = value
            value = value.astype(F32)
            total = total + jnp.sum(value * value, axis=1, keepdims=True)
        scale = lax.rsqrt(total / WIDTH + EPS)
        for side in range(2):
            value = mid[side, rows_of(s), :].astype(F32) * scale * gains[side]
            normed[rows_of(s), side * HALF : (side + 1) * HALF] = value.astype(BF16)

    def hidden_of(up_raw, gate_raw, columns):
        taps = conv_taps[:, columns]
        ups = up_scale[columns].reshape(1, -1)
        gates = gate_scale[columns].reshape(1, -1)
        lifted = (up_raw * ups).astype(BF16).astype(F32)
        at = lax.broadcasted_iota(jnp.int32, lifted.shape, 0)
        before = jnp.where(at == 0, 0.0, pltpu.roll(lifted, 1, 0))
        after = jnp.where(at == LENGTH - 1, 0.0, pltpu.roll(lifted, LENGTH - 1, 0))
        conv = taps[0:1] * before + taps[1:2] * lifted + taps[2:3] * after
        return (jax.nn.gelu(conv) * (gate_raw * gates)).astype(BF16)

    def slab(u):
        return w[u].reshape(WIDTH, PAIR)

    def feed_up(j):
        raw[...] = jnp.dot(normed[...], slab(U_FF + 2 * j), preferred_element_type=F32)

    def feed_gate(j):
        gate_raw = jnp.dot(normed[...], slab(U_FF + 2 * j + 1), preferred_element_type=F32)
        columns = block_of(j)
        for s in range(SEQS):
            part_rows = slice(s * LENGTH, (s + 1) * LENGTH)
            hid[part_rows, columns] = hidden_of(raw[part_rows, :], gate_raw[part_rows], columns)

    def feed_last(_):
        both = jnp.dot(normed[...], slab(U_LAST), preferred_element_type=F32)
        columns = pl.ds(10 * LANES, LANES)
        for s in range(SEQS):
            some = both[s * LENGTH : (s + 1) * LENGTH]
            hid[s * LENGTH : (s + 1) * LENGTH, columns] = hidden_of(
                some[:, :LANES], some[:, LANES:], columns
            )

    def down_first(n):
        side, block = n // 4, lax.rem(n, 4)
        right = jnp.concatenate(
            [w[U_DOWN + k, side, block].reshape(256, PAIR) for k in range(FIRST_K)], axis=1
        )
        acc[:, block_of(n)] = dot_nt(hid[:, 0 : FIRST_K * PAIR], right)

    def down_rest(side, block):
        right = [w[U_DOWN + k, side, block].reshape(256, PAIR) for k in range(FIRST_K, 5)]
        right = jnp.concatenate(right + [w_end[side, block].reshape(256, LANES)], axis=1)
        total = acc[:, block_of(side * 4 + block)] + dot_nt(hid[:, FIRST_K * PAIR : HID], right)
        part[side, :, block_of(block)] = total.astype(BF16)

    def compute(m):
        start = 0
        starts = {}
        for name, count in PIECES:
            starts[name] = (start, count)
            start += count

        def during(name, body):
            first_one, count = starts[name]

            @pl.when((m >= first_one) & (m < first_one + count))
            def _():
                body(m - first_one)

        def share(_):
            for load in loads[5:]:
                load.wait()
            across(x_hbm, x.at[tp], X_INPUT).start()
            across(gain_hbm, mate_gain, X_GAIN).start()
            across(out_scale_hbm, mate_out_scale, X_SCALE).start()

        def pooling(s):
            @pl.when(s == 0)
            def _():
                across(x_hbm, x.at[mate], X_INPUT).wait_recv()
                across(gain_hbm, mate_gain, X_GAIN).wait_recv()
                across(out_scale_hbm, mate_out_scale, X_SCALE).wait_recv()

            pool(s)

        def projecting(k):
            side = jnp.where(k < 4, mate, tp)
            block = lax.rem(k, 4)
            project(side, block)
            mixer_piece(side, block).start()

        def norming(s):
            @pl.when(s == 0)
            def _():
                for side in (mate, tp):
                    for block in range(4):
                        mixer_piece(side, block).wait_recv()

            norm(s)

        def feeding(k):
            @pl.when(lax.rem(k, 2) == 0)
            def _():
                feed_up(k // 2)

            @pl.when(lax.rem(k, 2) == 1)
            def _():
                feed_gate(k // 2)

        during("share", share)
        during("pool", pooling)
        during("group", group)
        during("project", projecting)
        during("norm", norming)
        during("feed", feeding)
        during("last", feed_last)
        during("down", down_first)

    def micro(m, _):
        def among(low, high):
            if high - low == 1:
                gather(low)
                return
            half = (low + high) // 2
            pl.when(m < half)(lambda: among(low, half))
            pl.when(m >= half)(lambda: among(half, high))

        among(0, TOTAL)
        compute(m)
        return 0

    lax.fori_loop(0, TOTAL, micro, 0)
    gather(TOTAL)

    for side in (mate, tp):
        for block in range(4):
            mixer_piece(side, block).wait_send()

    def first_half(block, _):
        down_rest(mate, block)
        final_piece(block).start()
        return 0

    lax.fori_loop(0, 4, first_half, 0)

    def second_half(block, _):
        columns = block_of(block)
        down_rest(tp, block)
        final_piece(block).wait_recv()

        def finish(s, _):
            total = part[tp, rows_of(s), columns].astype(F32) + end[rows_of(s), columns].astype(F32)
            scale = down_scale[columns].reshape(1, PAIR)
            value = mid[tp, rows_of(s), columns].astype(F32) + total * scale
            x[tp, rows_of(s), columns] = value.astype(BF16)
            return 0

        lax.fori_loop(0, SEQS, finish, 0)
        pltpu.make_async_copy(x.at[tp, :, columns], y.at[:, columns], y_sem.at[block]).start()
        return 0

    lax.fori_loop(0, 4, second_half, 0)

    across(x_hbm, x.at[tp], X_INPUT).wait_send()
    across(gain_hbm, mate_gain, X_GAIN).wait_send()
    across(out_scale_hbm, mate_out_scale, X_SCALE).wait_send()
    for block in range(4):
        final_piece(block).wait_send()
    for k in range(U_END // SEND_GROUP + 1):
        lanes = PAIR if k == U_END // SEND_GROUP else 2 * PAIR * SEND_GROUP
        ref = normed.at[pl.ds(0, 31 * 32), pl.ds(0, lanes)]
        pltpu.make_async_copy(ref, ref, send_sem.at[k]).wait()
    for block in range(4):
        columns = block_of(block)
        pltpu.make_async_copy(x.at[tp, :, columns], y.at[:, columns], y_sem.at[block]).wait()


def layer(
    layer_in,
    mix_gain,
    pool_weight,
    pool_scale,
    out_weight,
    out_scale,
    channel_gain,
    up_weight,
    up_scale,
    gate_weight,
    gate_scale,
    conv_weight,
    down_weight,
    down_scale,
):
    anywhere = pl.BlockSpec(memory_space=pl.ANY)
    dma = pltpu.SemaphoreType.DMA
    return pl.pallas_call(
        kernel,
        out_shape=jax.ShapeDtypeStruct((ROWS, HALF), BF16),
        in_specs=[anywhere] * 14,
        out_specs=anywhere,
        scratch_shapes=[
            pltpu.VMEM((U_END, 2, 4, 4, 64, PAIR), BF16),
            pltpu.VMEM((2, 4, 4, 64, LANES), BF16),
            pltpu.VMEM((2, ROWS, HALF), BF16),
            pltpu.VMEM((2, ROWS, HALF), BF16),
            pltpu.VMEM((2, ROWS, HALF), BF16),
            pltpu.VMEM((ROWS, HALF), BF16),
            pltpu.VMEM((2, ROWS, HALF), BF16),
            pltpu.VMEM((ROWS, WIDTH), BF16),
            pltpu.VMEM((ROWS, HID), BF16),
            pltpu.VMEM((ROWS, WIDTH), F32),
            pltpu.VMEM((ROWS, PAIR), F32),
            pltpu.VMEM((2, 16, 512), F32),
            pltpu.VMEM((64, HALF), F32),
            pltpu.VMEM((64, HID), F32),
            pltpu.VMEM((64, HID), F32),
            pltpu.VMEM((64, HID), F32),
            pltpu.VMEM((HALF,), BF16),
            pltpu.VMEM((2, 512), F32),
            pltpu.VMEM((HALF,), F32),
            pltpu.VMEM((HALF,), F32),
            pltpu.VMEM((HALF,), BF16),
            pltpu.VMEM((HALF,), BF16),
            pltpu.VMEM((HID,), F32),
            pltpu.VMEM((HID,), F32),
            pltpu.VMEM((3, HID), F32),
            pltpu.VMEM((HALF,), F32),
            dma((14,)),
            dma((U_END // SEND_GROUP + 1,)),
            dma((UNITS, STAGES)),
            dma((15,)),
            dma((15,)),
            dma((4,)),
        ],
        compiler_params=pltpu.CompilerParams(
            collective_id=0, has_side_effects=True, vmem_limit_bytes=66_000_000
        ),
    )(
        layer_in,
        pool_weight.transpose(0, 2, 1),
        out_weight.T,
        up_weight,
        gate_weight,
        down_weight.T,
        mix_gain,
        pool_scale,
        out_scale,
        channel_gain,
        up_scale,
        gate_scale,
        conv_weight,
        down_scale,
    )


def solution(mesh):
    torus = Mesh(
        mesh.devices.reshape(mesh.shape["rep"], 2, 4, 4, mesh.shape["tp"]),
        ("rep", "fs_0", "fs_1", "fs_2", "tp"),
    )
    in_specs = (
        P(REP_FS, "tp"),
        P("tp"),
        P("tp", None, FS),
        P("tp", None),
        P("tp", FS),
        P("tp"),
        P("tp"),
        P(FS, "tp"),
        P("tp"),
        P(FS, "tp"),
        P("tp"),
        P(None, "tp"),
        P("tp", FS),
        P("tp"),
    )
    out_specs = P(REP_FS, "tp")
    return jax.shard_map(
        layer, mesh=torus, in_specs=in_specs, out_specs=out_specs, check_vma=False
    )
```

```python
import jax
import jax.numpy as jnp
from jax import lax
from jax.experimental import pallas as pl
from jax.experimental.pallas import tpu as pltpu
from jax.sharding import Mesh
from jax.sharding import PartitionSpec as P

LENGTH = 256
FS = ("fs_0", "fs_1", "fs_2")
REP_FS = ("rep", "fs_0", "fs_1", "fs_2")
EPS = 1e-06

F32 = jnp.float32
BF16 = jnp.bfloat16
MESH = pl.DeviceIdType.MESH

ROWS = 1024
HALF = 1024
WIDTH = 2048
HID = 1408
SEQS = ROWS // LENGTH
LANES = 128
PAIR = 2 * LANES

U_POOL = 0
U_OUT = 1
U_LAST = 5
U_FF = 6
U_DOWN = 16
U_TILE = 19
UNITS = 24
TILES = UNITS - U_TILE
STAGES = 5
SEND_GROUP = 4
FIRST = (U_TILE - U_DOWN) * PAIR

ORDERS = (
    "yzx",
    "xyz",
    "xzy",
    "xzy",
    "yxz",
    "yzx",
    "xzy",
    "yxz",
    "yzx",
    "xyz",
    "xyz",
    "yxz",
    "yzx",
    "yxz",
    "yxz",
    "xzy",
    "yxz",
    "xzy",
    "xzy",
    "xzy",
    "yxz",
    "yzx",
    "yzx",
    "yxz",
)

SCHEDULE = (
    (16, 24, 48, 32, 128, 0,),
    (
        8, 56, 120, 96, 144, 88, 72, 160, 64, 136, 1016, 1032, 33, 17, 104, 1024, 25, 1128, 152,
        129, 1048, 49, 1000, 1,
    ),
    (1008, 1056, 9, 80, 57, 112,),
    (1120, 1096, 1144, 121, 145, 97, 184,),
    (1088, 1160, 1072, 73, 161, 89, 40,),
    (
        1064, 1136, 1033, 1017, 137, 34, 65, 176, 168, 18, 1025, 1104, 26, 105, 1152, 1129, 1049,
        1001, 1009, 10, 1057, 2, 58, 1080, 1112, 1121, 1097, 1145, 1184, 1161, 122, 1073, 1089,
        1137, 74, 1040, 1065, 50, 90, 1176, 1018, 1168, 1105, 146, 1026, 1034, 41, 19, 98, 35, 1002,
        1010, 138, 3, 1122, 1058, 66, 1050, 1074, 1041, 42, 1146, 1090, 75, 1098, 1035, 36, 11, 59,
        1138, 27, 81, 1066, 91, 1019, 1042, 153, 106, 1075, 76, 1003, 1011, 1059, 4, 1081, 185, 20,
        1091, 1153, 1036, 99, 82, 12, 1106, 1027, 1185, 28, 1004,
    ),
    (1020, 1076,),
    (107, 169, 177, 154, 113, 51, 60, 67, 1082, 1099, 1028, 1169, 1012,),
    (1177, 1113, 1154, 1107,),
    (100, 83, 108,),
    (),
    (139,),
    (114,),
    (),
    (1051, 1060, 1067,),
    (92, 68, 1083, 52, 1100,),
    (130,),
    (123,),
    (1108, 1114,),
    (1139, 115, 84, 162, 1068, 43, 1052,),
    (147,),
    (1092, 1130, 1115, 178,),
    (1162, 170, 116,),
    (1123, 131, 124, 163, 1084,),
    (1178, 1170, 186,),
    (1043, 44, 140,),
    (1147, 1131, 179, 132,),
    (1163, 1186, 148, 1124, 1116,),
    (187, 171, 155,),
    (1044, 1140, 164,),
    (1179, 180, 1148, 1187, 188, 1132,),
    (),
    (),
    (1155, 1171, 172, 156,),
    (1164,),
    (1180,),
    (),
    (),
    (1188, 1172, 1156,),
)

PIECES = (
    ("share", 1),
    ("pool", 4),
    ("group", 2),
    ("project", 8),
    ("norm", 4),
    ("feed", 10),
    ("last", 1),
    ("down", 8),
)
TOTAL = sum(count for _, count in PIECES)

AXIS = {"x": "fs_2", "y": "fs_1"}

X_GAIN, X_SCALE, X_INPUT, X_MIXER, X_FINAL = 0, 1, 2, 3, 4


def steps_of(order):
    steps = []
    for phase, dim in enumerate(order):
        steps += [(phase, "a")] if dim == "z" else [(phase, "a"), (phase, "b")]
    return steps


def shards_in(order, stage):
    phase, step = steps_of(order)[stage]
    held = 1
    for dim in order[:phase]:
        held *= 2 if dim == "z" else 4
    return held if order[phase] == "z" or step == "b" else 2 * held


def group_of(u):
    return -(-U_TILE // SEND_GROUP) if u >= U_TILE else u // SEND_GROUP


def dot_nt(left, right):
    return lax.dot_general(left, right, (((1,), (1,)), ((), ())), preferred_element_type=F32)


def kernel(
    x_hbm,
    pool_hbm,
    out_hbm,
    up_hbm,
    gate_hbm,
    down_hbm,
    mix_gain_hbm,
    pool_scale_hbm,
    out_scale_hbm,
    gain_hbm,
    up_scale_hbm,
    gate_scale_hbm,
    conv_hbm,
    down_scale_hbm,
    y,
    w,
    w_tile,
    x,
    part,
    got,
    end,
    mid,
    normed,
    hid,
    acc,
    raw,
    st_pool,
    st_out,
    st_up,
    st_gate,
    st_down,
    mix_gain,
    pool_scale,
    out_scale,
    mate_out_scale,
    gain,
    mate_gain,
    up_scale,
    gate_scale,
    conv_taps,
    down_scale,
    in_sem,
    send_sem,
    recv_sem,
    tp_send,
    tp_recv,
):
    rep = lax.axis_index("rep")
    zl = lax.axis_index("fs_0")
    me = {"z": zl, "y": lax.axis_index("fs_1"), "x": lax.axis_index("fs_2")}
    tp = lax.axis_index("tp")
    mate = 1 - tp
    zz = rep * 2 + zl
    z_up = lax.rem(zz + 1, 4)
    z_down = lax.rem(zz + 3, 4)

    def to_z(place):
        return {"rep": place // 2, "fs_0": lax.rem(place, 2)}

    def ring(dim, shift):
        return lax.rem(me[dim] + shift + 4, 4)

    peers = [to_z(z_up), to_z(z_down), {"tp": mate}]
    for dim in ("x", "y"):
        peers += [{AXIS[dim]: ring(dim, 1)}, {AXIS[dim]: ring(dim, -1)}]

    barrier = pltpu.get_barrier_semaphore()
    for peer in peers:
        pl.semaphore_signal(barrier, inc=1, device_id=peer, device_id_type=MESH)

    loads = [
        pltpu.make_async_copy(src, dst, in_sem.at[k])
        for k, (src, dst) in enumerate(
            (
                (pool_hbm, st_pool),
                (out_hbm, st_out),
                (up_hbm, st_up),
                (gate_hbm, st_gate),
                (down_hbm, st_down),
                (x_hbm, x.at[tp]),
                (mix_gain_hbm, mix_gain),
                (pool_scale_hbm, pool_scale),
                (out_scale_hbm, out_scale),
                (gain_hbm, gain),
                (up_scale_hbm, up_scale),
                (gate_scale_hbm, gate_scale),
                (conv_hbm, conv_taps),
                (down_scale_hbm, down_scale),
            )
        )
    ]
    for load in loads[:5]:
        load.start()
    for load in loads[:5]:
        load.wait()

    mine = (me["z"], me["y"], me["x"])
    for g in range(2):
        for ct in range(4):
            block = st_pool[g, :, ct * LANES : (ct + 1) * LANES]
            lanes = pl.ds(g * LANES, LANES)
            w[(U_POOL, *mine, pl.ds(ct * 16, 16), lanes)] = block.astype(BF16)
    for k in range(4):
        w[(U_OUT + k, *mine)] = st_out[:, k * PAIR : (k + 1) * PAIR].astype(BF16)
    for k in range(5):
        columns = slice(k * PAIR, (k + 1) * PAIR)
        w[(U_FF + 2 * k, *mine)] = st_up[:, columns].astype(BF16)
        w[(U_FF + 2 * k + 1, *mine)] = st_gate[:, columns].astype(BF16)
    rest = slice(10 * LANES, HID)
    w[(U_LAST, *mine, slice(None), pl.ds(0, LANES))] = st_up[:, rest].astype(BF16)
    w[(U_LAST, *mine, slice(None), pl.ds(LANES, LANES))] = st_gate[:, rest].astype(BF16)
    for k in range(U_TILE - U_DOWN):
        w[(U_DOWN + k, *mine)] = st_down[:, k * PAIR : (k + 1) * PAIR].astype(BF16)
    for k in range(TILES):
        columns = slice(FIRST + k * LANES, FIRST + (k + 1) * LANES)
        w_tile[(k, *mine)] = st_down[:, columns].astype(BF16)
    for load in loads[5:]:
        load.start()

    pl.semaphore_wait(barrier, len(peers))

    def across(src, dst, index):
        return pltpu.make_async_remote_copy(
            src_ref=src,
            dst_ref=dst,
            send_sem=tp_send.at[index],
            recv_sem=tp_recv.at[index],
            device_id={"tp": mate},
            device_id_type=MESH,
        )

    def region(u, order, phase, place, rows):
        picks = {}
        for k, dim in enumerate(order):
            if k < phase:
                picks[dim] = slice(None)
            elif k == phase:
                picks[dim] = pl.ds(place, 1)
            else:
                picks[dim] = pl.ds(me[dim], 1)
        where = (picks["z"], picks["y"], picks["x"], rows, slice(None))
        return w_tile.at[(u - U_TILE, *where)] if u >= U_TILE else w.at[(u, *where)]

    every, first, second = pl.ds(0, 64), pl.ds(0, 32), pl.ds(32, 32)

    def moves(u, stage):
        order = ORDERS[u]
        phase, step = steps_of(order)[stage]
        dim = order[phase]
        if dim == "z":
            return phase, ((zl, first, to_z(z_up)), (zl, second, to_z(z_down)))
        right, left = {AXIS[dim]: ring(dim, 1)}, {AXIS[dim]: ring(dim, -1)}
        if step == "a":
            return phase, ((me[dim], every, right), (me[dim], every, left))
        return phase, ((ring(dim, -1), first, right), (ring(dim, 1), second, left))

    def send(u, stage):
        phase, both = moves(u, stage)
        for place, rows, peer in both:
            ref = region(u, ORDERS[u], phase, place, rows)
            pltpu.make_async_remote_copy(
                src_ref=ref,
                dst_ref=ref,
                send_sem=send_sem.at[group_of(u)],
                recv_sem=recv_sem.at[u, stage],
                device_id=peer,
                device_id_type=MESH,
            ).start()

    def arrived(u, stage):
        count = shards_in(ORDERS[u], stage)
        box = {1: (1, 1, 1), 2: (1, 1, 2), 4: (1, 1, 4), 8: (1, 2, 4), 16: (1, 4, 4)}[count]
        where = tuple(pl.ds(0, size) for size in box)
        ref = w_tile.at[(u - U_TILE, *where)] if u >= U_TILE else w.at[(u, *where)]
        pltpu.make_async_copy(ref, ref, recv_sem.at[u, stage]).wait()

    def gather(position):
        for code in SCHEDULE[position]:
            u, stage = divmod(code % 1000, 8)
            (arrived if code >= 1000 else send)(u, stage)

    def row(ref):
        return ref[...].astype(F32).reshape(1, ref.shape[0])

    def rows_of(s):
        return pl.ds(pl.multiple_of(s * LENGTH, LENGTH), LENGTH)

    def block_of(n):
        return pl.ds(pl.multiple_of(n * PAIR, PAIR), PAIR)

    mixed = hid

    def pool(s):
        total = jnp.zeros((LENGTH, 1), F32)
        for side in range(2):
            values = x[side, rows_of(s), :].astype(F32)
            total = total + jnp.sum(values * values, axis=1, keepdims=True)
        scale = lax.rsqrt(total / WIDTH + EPS)
        at = lax.broadcasted_iota(jnp.int32, (LENGTH, LENGTH), 0)
        col = lax.broadcasted_iota(jnp.int32, (LENGTH, LENGTH), 1)
        for g in range(2):
            reach = jnp.where(tp == 0, 1 << g, 4 << g)
            lower = jnp.maximum(at - reach, 0)
            upper = jnp.minimum(at + reach, LENGTH)
            band = jnp.where((col >= lower) & (col < upper), 1.0, 0.0).astype(BF16)
            count = (upper[:, :1] - lower[:, :1]).astype(F32)
            columns = slice(g * 512, (g + 1) * 512)
            piece = x[tp, rows_of(s), columns].astype(F32) * scale * row(mix_gain)[:, columns]
            piece = piece.astype(BF16)
            window = jnp.dot(band, piece, preferred_element_type=F32)
            mixed[rows_of(s), columns] = (window / count - piece.astype(F32)).astype(BF16)

    def group(g):
        columns = pl.ds(pl.multiple_of(g * 512, 512), 512)
        lanes = pl.ds(pl.multiple_of(g * LANES, LANES), LANES)
        maps = w[U_POOL, :, :, :, :, lanes].reshape(32, 4, 16, LANES)
        right = jnp.concatenate([maps[:, ct].reshape(512, LANES) for ct in range(4)], axis=1)
        out = dot_nt(mixed[:, columns], right) * pool_scale[pl.ds(g, 1), :]
        normed[:, columns] = out.astype(BF16)

    def project(side, block):
        right = jnp.concatenate(
            [w[U_OUT + k, side, block].reshape(256, PAIR) for k in range(4)], axis=1
        )
        part[side, :, block_of(block)] = dot_nt(normed[:, 0:HALF], right).astype(BF16)

    def mixer_piece(side, block):
        columns = block_of(block)
        return across(part.at[side, :, columns], got.at[side, :, columns], X_MIXER)

    def final_piece(block):
        columns = block_of(block)
        return across(part.at[mate, :, columns], end.at[:, columns], X_FINAL + block)

    def norm(s):
        ours, theirs = row(gain), row(mate_gain)
        gains = (jnp.where(tp == 0, ours, theirs), jnp.where(tp == 0, theirs, ours))
        ours, theirs = row(out_scale), row(mate_out_scale)
        scales = (jnp.where(tp == 0, ours, theirs), jnp.where(tp == 0, theirs, ours))
        total = jnp.zeros((LENGTH, 1), F32)
        for side in range(2):
            added = part[side, rows_of(s), :].astype(F32) + got[side, rows_of(s), :].astype(F32)
            value = x[side, rows_of(s), :].astype(F32) + added * scales[side]
            value = value.astype(BF16)
            mid[side, rows_of(s), :] = value
            value = value.astype(F32)
            total = total + jnp.sum(value * value, axis=1, keepdims=True)
        scale = lax.rsqrt(total / WIDTH + EPS)
        for side in range(2):
            value = mid[side, rows_of(s), :].astype(F32) * scale * gains[side]
            normed[rows_of(s), side * HALF : (side + 1) * HALF] = value.astype(BF16)

    def activation(up_raw, columns):
        taps = conv_taps[:, columns]
        ups = up_scale[columns].reshape(1, -1)
        lifted = (up_raw * ups).astype(BF16).astype(F32)
        at = lax.broadcasted_iota(jnp.int32, lifted.shape, 0)
        before = jnp.where(at == 0, 0.0, pltpu.roll(lifted, 1, 0))
        after = jnp.where(at == LENGTH - 1, 0.0, pltpu.roll(lifted, LENGTH - 1, 0))
        return jax.nn.gelu(taps[0:1] * before + taps[1:2] * lifted + taps[2:3] * after)

    def hidden_of(active, gate_raw, columns):
        return (active * (gate_raw * gate_scale[columns].reshape(1, -1))).astype(BF16)

    def slab(u):
        return w[u].reshape(WIDTH, PAIR)

    def feed_up(j):
        raw[...] = jnp.dot(normed[...], slab(U_FF + 2 * j), preferred_element_type=F32)

    def feed_gate(j):
        columns = block_of(j)
        for s in range(SEQS):
            some = slice(s * LENGTH, (s + 1) * LENGTH)
            raw[some, :] = activation(raw[some, :], columns)
        gate_raw = jnp.dot(normed[...], slab(U_FF + 2 * j + 1), preferred_element_type=F32)
        hid[:, columns] = hidden_of(raw[...], gate_raw, columns)

    def feed_last(_):
        both = jnp.dot(normed[...], slab(U_LAST), preferred_element_type=F32)
        columns = pl.ds(10 * LANES, LANES)
        for s in range(SEQS):
            some = slice(s * LENGTH, (s + 1) * LENGTH)
            active = activation(both[some, :LANES], columns)
            hid[some, columns] = hidden_of(active, both[some, LANES:], columns)

    def down_first(n):
        side, block = n // 4, lax.rem(n, 4)
        right = jnp.concatenate(
            [w[u, side, block].reshape(256, PAIR) for u in range(U_DOWN, U_TILE)], axis=1
        )
        acc[:, block_of(n)] = dot_nt(hid[:, 0:FIRST], right)

    def down_rest(side, block):
        right = jnp.concatenate(
            [w_tile[k, side, block].reshape(256, LANES) for k in range(TILES)], axis=1
        )
        return acc[:, block_of(side * 4 + block)] + dot_nt(hid[:, FIRST:HID], right)

    def compute(m):
        start = 0
        starts = {}
        for name, count in PIECES:
            starts[name] = (start, count)
            start += count

        def during(name, body):
            first_one, count = starts[name]

            @pl.when((m >= first_one) & (m < first_one + count))
            def _():
                body(m - first_one)

        def share(_):
            for load in loads[5:]:
                load.wait()
            across(x_hbm, x.at[tp], X_INPUT).start()
            across(gain_hbm, mate_gain, X_GAIN).start()
            across(out_scale_hbm, mate_out_scale, X_SCALE).start()

        def pooling(s):
            @pl.when(s == 0)
            def _():
                across(x_hbm, x.at[mate], X_INPUT).wait_recv()
                across(gain_hbm, mate_gain, X_GAIN).wait_recv()
                across(out_scale_hbm, mate_out_scale, X_SCALE).wait_recv()

            pool(s)

        def projecting(k):
            side = jnp.where(k < 4, mate, tp)
            block = lax.rem(k, 4)
            project(side, block)
            mixer_piece(side, block).start()

        def norming(s):
            @pl.when(s == 0)
            def _():
                across(part, got, X_MIXER).wait_recv()

            norm(s)

        def feeding(k):
            @pl.when(lax.rem(k, 2) == 0)
            def _():
                feed_up(k // 2)

            @pl.when(lax.rem(k, 2) == 1)
            def _():
                feed_gate(k // 2)

        during("share", share)
        during("pool", pooling)
        during("group", group)
        during("project", projecting)
        during("norm", norming)
        during("feed", feeding)
        during("last", feed_last)
        during("down", down_first)

    def micro(m, _):
        def among(low, high):
            if high - low == 1:
                gather(low)
                return
            half = (low + high) // 2
            pl.when(m < half)(lambda: among(low, half))
            pl.when(m >= half)(lambda: among(half, high))

        among(0, TOTAL)
        compute(m)
        return 0

    lax.fori_loop(0, TOTAL, micro, 0)
    gather(TOTAL)

    across(part, got, X_MIXER).wait_send()

    def first_half(block, _):
        part[mate, :, block_of(block)] = down_rest(mate, block).astype(BF16)
        final_piece(block).start()
        return 0

    lax.fori_loop(0, 4, first_half, 0)

    def second_half(block, _):
        columns = block_of(block)
        final_piece(block).wait_recv()
        total = down_rest(tp, block).astype(BF16).astype(F32) + end[:, columns].astype(F32)
        scale = down_scale[columns].reshape(1, PAIR)
        y[:, columns] = (mid[tp, :, columns].astype(F32) + total * scale).astype(BF16)
        return 0

    lax.fori_loop(0, 4, second_half, 0)

    across(x_hbm, x.at[tp], X_INPUT).wait_send()
    across(gain_hbm, mate_gain, X_GAIN).wait_send()
    across(out_scale_hbm, mate_out_scale, X_SCALE).wait_send()
    for block in range(4):
        final_piece(block).wait_send()
    full, over = divmod(U_TILE, SEND_GROUP)
    lanes = [2 * PAIR * SEND_GROUP] * full + [2 * PAIR * over, PAIR * TILES]
    for k in range(full + 2):
        ref = normed.at[pl.ds(0, 31 * 32), pl.ds(0, lanes[k])]
        pltpu.make_async_copy(ref, ref, send_sem.at[k]).wait()


def layer(
    layer_in,
    mix_gain,
    pool_weight,
    pool_scale,
    out_weight,
    out_scale,
    channel_gain,
    up_weight,
    up_scale,
    gate_weight,
    gate_scale,
    conv_weight,
    down_weight,
    down_scale,
):
    anywhere = pl.BlockSpec(memory_space=pl.ANY)
    dma = pltpu.SemaphoreType.DMA
    return pl.pallas_call(
        kernel,
        out_shape=pltpu.VMEM((ROWS, HALF), BF16),
        in_specs=[anywhere] * 14,
        out_specs=pl.BlockSpec(memory_space=pltpu.VMEM),
        scratch_shapes=[
            pltpu.VMEM((U_TILE, 2, 4, 4, 64, PAIR), BF16),
            pltpu.VMEM((TILES, 2, 4, 4, 64, LANES), BF16),
            pltpu.VMEM((2, ROWS, HALF), BF16),
            pltpu.VMEM((2, ROWS, HALF), BF16),
            pltpu.VMEM((2, ROWS, HALF), BF16),
            pltpu.VMEM((ROWS, HALF), BF16),
            pltpu.VMEM((2, ROWS, HALF), BF16),
            pltpu.VMEM((ROWS, WIDTH), BF16),
            pltpu.VMEM((ROWS, HID), BF16),
            pltpu.VMEM((ROWS, WIDTH), F32),
            pltpu.VMEM((ROWS, PAIR), F32),
            pltpu.VMEM((2, 16, 512), F32),
            pltpu.VMEM((64, HALF), F32),
            pltpu.VMEM((64, HID), F32),
            pltpu.VMEM((64, HID), F32),
            pltpu.VMEM((64, HID), F32),
            pltpu.VMEM((HALF,), BF16),
            pltpu.VMEM((2, 512), F32),
            pltpu.VMEM((HALF,), F32),
            pltpu.VMEM((HALF,), F32),
            pltpu.VMEM((HALF,), BF16),
            pltpu.VMEM((HALF,), BF16),
            pltpu.VMEM((HID,), F32),
            pltpu.VMEM((HID,), F32),
            pltpu.VMEM((3, HID), F32),
            pltpu.VMEM((HALF,), F32),
            dma((14,)),
            dma((group_of(U_TILE) + 1,)),
            dma((UNITS, STAGES)),
            dma((8,)),
            dma((8,)),
        ],
        compiler_params=pltpu.CompilerParams(
            collective_id=0, has_side_effects=True, vmem_limit_bytes=63_500_000
        ),
    )(
        layer_in,
        pool_weight.transpose(0, 2, 1),
        out_weight.T,
        up_weight,
        gate_weight,
        down_weight.T,
        mix_gain,
        pool_scale,
        out_scale,
        channel_gain,
        up_scale,
        gate_scale,
        conv_weight,
        down_scale,
    )


def solution(mesh):
    torus = Mesh(
        mesh.devices.reshape(mesh.shape["rep"], 2, 4, 4, mesh.shape["tp"]),
        ("rep", "fs_0", "fs_1", "fs_2", "tp"),
    )
    in_specs = (
        P(REP_FS, "tp"),
        P("tp"),
        P("tp", None, FS),
        P("tp", None),
        P("tp", FS),
        P("tp"),
        P("tp"),
        P(FS, "tp"),
        P("tp"),
        P(FS, "tp"),
        P("tp"),
        P(None, "tp"),
        P("tp", FS),
        P("tp"),
    )
    out_specs = P(REP_FS, "tp")
    return jax.shard_map(
        layer, mesh=torus, in_specs=in_specs, out_specs=out_specs, check_vma=False
    )
```

```python
import jax
import jax.numpy as jnp
from jax import lax
from jax.experimental import pallas as pl
from jax.experimental.pallas import tpu as pltpu
from jax.sharding import Mesh
from jax.sharding import PartitionSpec as P

LENGTH = 256
FS = ("fs_0", "fs_1", "fs_2")
REP_FS = ("rep", "fs_0", "fs_1", "fs_2")
EPS = 1e-06

F32 = jnp.float32
BF16 = jnp.bfloat16
MESH = pl.DeviceIdType.MESH

ROWS = 1024
HALF = 1024
WIDTH = 2048
HID = 1408
SEQS = ROWS // LENGTH
LANES = 128
PAIR = 2 * LANES

U_POOL = 0
U_OUT = 1
U_LAST = 5
U_FF = 6
U_DOWN = 16
U_TILE = 19
UNITS = 24
TILES = UNITS - U_TILE
STAGES = 5
SEND_GROUP = 4
FIRST = (U_TILE - U_DOWN) * PAIR

ORDERS = (
    "yzx",
    "yxz",
    "yxz",
    "yxz",
    "xzy",
    "yxz",
    "xyz",
    "xzy",
    "xzy",
    "yzx",
    "xzy",
    "xzy",
    "yxz",
    "yxz",
    "xzy",
    "yzx",
    "yzx",
    "yxz",
    "xyz",
    "zyx",
    "yxz",
    "yxz",
    "xzy",
    "xzy",
)

SCHEDULE = (
    (80, 48, 32, 144, 24, 0, 16, 168, 40, 152,),
    (
        112, 8, 56, 96, 88, 72, 184, 1152, 176, 160, 1080, 1024, 81, 25, 64, 128, 1048, 1000, 49, 1,
        1032, 1016, 33, 17, 1168, 169, 1144, 145, 104,
    ),
    (1040, 1112, 1008, 113, 41, 9,),
    (1056, 1096, 1088, 89, 57, 97, 136,),
    (1184, 1072, 1176, 1160, 1081, 1025, 26, 161, 73, 120, 82,),
    (
        1064, 1128, 1049, 1001, 177, 65, 129, 50, 2, 1033, 34, 185, 1017, 18, 1169, 1145, 1113, 114,
        1104, 1089, 1041, 1057, 1009, 90, 1097, 146, 1082, 1136, 1161, 10, 1073, 58, 1002, 1120,
        1026, 1129, 1177, 1065, 130, 1185, 83, 1034, 27, 186, 1114, 66, 1050, 3, 1018, 1090, 74,
        1058, 178, 1146, 1010, 137, 1130, 121, 35, 1186, 1027, 28, 19, 1066, 11, 1074, 1178, 1083,
        42, 1137, 1121, 122, 84, 1003, 4, 1019, 20, 147, 1011, 1028, 75, 105, 51, 1035, 1122, 12,
        36, 1042, 1084, 67, 1004,
    ),
    (1147, 1105, 43,),
    (1020, 1051, 138, 52, 1036, 98, 153, 1075, 59, 1043, 1012,),
    (76, 44,),
    (),
    (1138,),
    (1067, 1153, 139,),
    (91,),
    (1098, 99,),
    (1052, 131, 148,),
    (1076, 1059, 1139,),
    (60,),
    (1099, 1044, 106,),
    (140,),
    (68,),
    (1091, 170,),
    (1131, 132, 92, 1148, 1060,),
    (1106, 107, 154, 115, 100, 162, 1068,),
    (1170, 171,),
    (1140, 1092, 1132, 1154, 123,),
    (1107, 187, 108,),
    (1162, 1171,),
    (163, 179,),
    (1100, 155,),
    (1115, 172,),
    (116,),
    (),
    (),
    (1187,),
    (1123, 124, 188,),
    (1163, 1108, 164,),
    (1179, 1155, 156, 180, 1172, 1116,),
    (1124, 1188,),
    (1164, 1156, 1180,),
)

PIECES = (
    ("share", 1),
    ("pool", 4),
    ("group", 2),
    ("project", 8),
    ("norm", 4),
    ("last", 1),
    ("feed", 6),
    ("down", 8),
    ("feed again", 4),
)
TOTAL = sum(count for _, count in PIECES)

AXIS = {"x": "fs_2", "y": "fs_1"}

X_GAIN, X_SCALE, X_INPUT, X_MIXER, X_FINAL = 0, 1, 2, 3, 4


def steps_of(order):
    steps = []
    for phase, dim in enumerate(order):
        steps += [(phase, "a")] if dim == "z" else [(phase, "a"), (phase, "b")]
    return steps


def shards_in(order, stage):
    phase, step = steps_of(order)[stage]
    held = 1
    for dim in order[:phase]:
        held *= 2 if dim == "z" else 4
    return held if order[phase] == "z" or step == "b" else 2 * held


def group_of(u):
    return -(-U_TILE // SEND_GROUP) if u >= U_TILE else u // SEND_GROUP


def dot_nt(left, right):
    return lax.dot_general(left, right, (((1,), (1,)), ((), ())), preferred_element_type=F32)


def kernel(
    x_hbm,
    pool_hbm,
    out_hbm,
    up_hbm,
    gate_hbm,
    down_hbm,
    mix_gain_hbm,
    pool_scale_hbm,
    out_scale_hbm,
    gain_hbm,
    up_scale_hbm,
    gate_scale_hbm,
    conv_hbm,
    down_scale_hbm,
    y,
    w,
    w_tile,
    x,
    part,
    got,
    end,
    mid,
    normed,
    hid,
    acc,
    raw,
    st_pool,
    st_out,
    st_up,
    st_gate,
    st_down,
    mix_gain,
    pool_scale,
    out_scale,
    mate_out_scale,
    gain,
    mate_gain,
    up_scale,
    gate_scale,
    conv_taps,
    down_scale,
    in_sem,
    send_sem,
    recv_sem,
    tp_send,
    tp_recv,
):
    rep = lax.axis_index("rep")
    zl = lax.axis_index("fs_0")
    me = {"z": zl, "y": lax.axis_index("fs_1"), "x": lax.axis_index("fs_2")}
    tp = lax.axis_index("tp")
    mate = 1 - tp
    zz = rep * 2 + zl
    z_up = lax.rem(zz + 1, 4)
    z_down = lax.rem(zz + 3, 4)

    def to_z(place):
        return {"rep": place // 2, "fs_0": lax.rem(place, 2)}

    def ring(dim, shift):
        return lax.rem(me[dim] + shift + 4, 4)

    peers = [to_z(z_up), to_z(z_down), {"tp": mate}]
    for dim in ("x", "y"):
        peers += [{AXIS[dim]: ring(dim, 1)}, {AXIS[dim]: ring(dim, -1)}]

    barrier = pltpu.get_barrier_semaphore()
    for peer in peers:
        pl.semaphore_signal(barrier, inc=1, device_id=peer, device_id_type=MESH)

    loads = [
        pltpu.make_async_copy(src, dst, in_sem.at[k])
        for k, (src, dst) in enumerate(
            (
                (pool_hbm, st_pool),
                (out_hbm, st_out),
                (up_hbm, st_up),
                (gate_hbm, st_gate),
                (down_hbm, st_down),
                (x_hbm, x.at[tp]),
                (mix_gain_hbm, mix_gain),
                (pool_scale_hbm, pool_scale),
                (out_scale_hbm, out_scale),
                (gain_hbm, gain),
                (up_scale_hbm, up_scale),
                (gate_scale_hbm, gate_scale),
                (conv_hbm, conv_taps),
                (down_scale_hbm, down_scale),
            )
        )
    ]
    for load in loads[:5]:
        load.start()
    for load in loads[:5]:
        load.wait()

    mine = (me["z"], me["y"], me["x"])
    for g in range(2):
        for ct in range(4):
            block = st_pool[g, :, ct * LANES : (ct + 1) * LANES]
            lanes = pl.ds(g * LANES, LANES)
            w[(U_POOL, *mine, pl.ds(ct * 16, 16), lanes)] = block.astype(BF16)
    for k in range(4):
        w[(U_OUT + k, *mine)] = st_out[:, k * PAIR : (k + 1) * PAIR].astype(BF16)
    for k in range(5):
        columns = slice(k * PAIR, (k + 1) * PAIR)
        w[(U_FF + 2 * k, *mine)] = st_up[:, columns].astype(BF16)
        w[(U_FF + 2 * k + 1, *mine)] = st_gate[:, columns].astype(BF16)
    rest = slice(10 * LANES, HID)
    w[(U_LAST, *mine, slice(None), pl.ds(0, LANES))] = st_up[:, rest].astype(BF16)
    w[(U_LAST, *mine, slice(None), pl.ds(LANES, LANES))] = st_gate[:, rest].astype(BF16)
    for k in range(U_TILE - U_DOWN):
        w[(U_DOWN + k, *mine)] = st_down[:, k * PAIR : (k + 1) * PAIR].astype(BF16)
    for k in range(TILES):
        columns = slice(FIRST + k * LANES, FIRST + (k + 1) * LANES)
        w_tile[(k, *mine)] = st_down[:, columns].astype(BF16)
    for load in loads[5:]:
        load.start()

    pl.semaphore_wait(barrier, len(peers))

    def across(src, dst, index):
        return pltpu.make_async_remote_copy(
            src_ref=src,
            dst_ref=dst,
            send_sem=tp_send.at[index],
            recv_sem=tp_recv.at[index],
            device_id={"tp": mate},
            device_id_type=MESH,
        )

    def region(u, order, phase, place, rows):
        picks = {}
        for k, dim in enumerate(order):
            if k < phase:
                picks[dim] = slice(None)
            elif k == phase:
                picks[dim] = pl.ds(place, 1)
            else:
                picks[dim] = pl.ds(me[dim], 1)
        where = (picks["z"], picks["y"], picks["x"], rows, slice(None))
        return w_tile.at[(u - U_TILE, *where)] if u >= U_TILE else w.at[(u, *where)]

    every, first, second = pl.ds(0, 64), pl.ds(0, 32), pl.ds(32, 32)

    def moves(u, stage):
        order = ORDERS[u]
        phase, step = steps_of(order)[stage]
        dim = order[phase]
        if dim == "z":
            return phase, ((zl, first, to_z(z_up)), (zl, second, to_z(z_down)))
        right, left = {AXIS[dim]: ring(dim, 1)}, {AXIS[dim]: ring(dim, -1)}
        if step == "a":
            return phase, ((me[dim], every, right), (me[dim], every, left))
        return phase, ((ring(dim, -1), first, right), (ring(dim, 1), second, left))

    def send(u, stage):
        phase, both = moves(u, stage)
        for place, rows, peer in both:
            ref = region(u, ORDERS[u], phase, place, rows)
            pltpu.make_async_remote_copy(
                src_ref=ref,
                dst_ref=ref,
                send_sem=send_sem.at[group_of(u)],
                recv_sem=recv_sem.at[u, stage],
                device_id=peer,
                device_id_type=MESH,
            ).start()

    def arrived(u, stage):
        count = shards_in(ORDERS[u], stage)
        box = {1: (1, 1, 1), 2: (1, 1, 2), 4: (1, 1, 4), 8: (1, 2, 4), 16: (1, 4, 4)}[count]
        where = tuple(pl.ds(0, size) for size in box)
        ref = w_tile.at[(u - U_TILE, *where)] if u >= U_TILE else w.at[(u, *where)]
        pltpu.make_async_copy(ref, ref, recv_sem.at[u, stage]).wait()

    def gather(position):
        for code in SCHEDULE[position]:
            u, stage = divmod(code % 1000, 8)
            (arrived if code >= 1000 else send)(u, stage)

    def row(ref):
        return ref[...].astype(F32).reshape(1, ref.shape[0])

    def rows_of(s):
        return pl.ds(pl.multiple_of(s * LENGTH, LENGTH), LENGTH)

    def block_of(n):
        return pl.ds(pl.multiple_of(n * PAIR, PAIR), PAIR)

    mixed = hid

    def pool(s):
        total = jnp.zeros((LENGTH, 1), F32)
        for side in range(2):
            values = x[side, rows_of(s), :].astype(F32)
            total = total + jnp.sum(values * values, axis=1, keepdims=True)
        scale = lax.rsqrt(total / WIDTH + EPS)
        at = lax.broadcasted_iota(jnp.int32, (LENGTH, LENGTH), 0)
        col = lax.broadcasted_iota(jnp.int32, (LENGTH, LENGTH), 1)
        for g in range(2):
            reach = jnp.where(tp == 0, 1 << g, 4 << g)
            lower = jnp.maximum(at - reach, 0)
            upper = jnp.minimum(at + reach, LENGTH)
            band = jnp.where((col >= lower) & (col < upper), 1.0, 0.0).astype(BF16)
            count = (upper[:, :1] - lower[:, :1]).astype(F32)
            columns = slice(g * 512, (g + 1) * 512)
            piece = x[tp, rows_of(s), columns].astype(F32) * scale * row(mix_gain)[:, columns]
            piece = piece.astype(BF16)
            window = jnp.dot(band, piece, preferred_element_type=F32)
            mixed[rows_of(s), columns] = (window / count - piece.astype(F32)).astype(BF16)

    def group(g):
        columns = pl.ds(pl.multiple_of(g * 512, 512), 512)
        lanes = pl.ds(pl.multiple_of(g * LANES, LANES), LANES)
        maps = w[U_POOL, :, :, :, :, lanes].reshape(32, 4, 16, LANES)
        right = jnp.concatenate([maps[:, ct].reshape(512, LANES) for ct in range(4)], axis=1)
        out = dot_nt(mixed[:, columns], right) * pool_scale[pl.ds(g, 1), :]
        normed[:, columns] = out.astype(BF16)

    def project(side, block):
        right = jnp.concatenate(
            [w[U_OUT + k, side, block].reshape(256, PAIR) for k in range(4)], axis=1
        )
        part[side, :, block_of(block)] = dot_nt(normed[:, 0:HALF], right).astype(BF16)

    def mixer_piece(side, block):
        columns = block_of(block)
        return across(part.at[side, :, columns], got.at[side, :, columns], X_MIXER)

    def final_piece(block):
        columns = block_of(block)
        return across(part.at[mate, :, columns], end.at[:, columns], X_FINAL + block)

    def norm(s):
        ours, theirs = row(gain), row(mate_gain)
        gains = (jnp.where(tp == 0, ours, theirs), jnp.where(tp == 0, theirs, ours))
        ours, theirs = row(out_scale), row(mate_out_scale)
        scales = (jnp.where(tp == 0, ours, theirs), jnp.where(tp == 0, theirs, ours))
        total = jnp.zeros((LENGTH, 1), F32)
        for side in range(2):
            added = part[side, rows_of(s), :].astype(F32) + got[side, rows_of(s), :].astype(F32)
            value = x[side, rows_of(s), :].astype(F32) + added * scales[side]
            value = value.astype(BF16)
            mid[side, rows_of(s), :] = value
            value = value.astype(F32)
            total = total + jnp.sum(value * value, axis=1, keepdims=True)
        scale = lax.rsqrt(total / WIDTH + EPS)
        for side in range(2):
            value = mid[side, rows_of(s), :].astype(F32) * scale * gains[side]
            normed[rows_of(s), side * HALF : (side + 1) * HALF] = value.astype(BF16)

    def activation(up_raw, columns):
        taps = conv_taps[:, columns]
        ups = up_scale[columns].reshape(1, -1)
        lifted = (up_raw * ups).astype(BF16).astype(F32)
        at = lax.broadcasted_iota(jnp.int32, lifted.shape, 0)
        before = jnp.where(at == 0, 0.0, pltpu.roll(lifted, 1, 0))
        after = jnp.where(at == LENGTH - 1, 0.0, pltpu.roll(lifted, LENGTH - 1, 0))
        return jax.nn.gelu(taps[0:1] * before + taps[1:2] * lifted + taps[2:3] * after)

    def hidden_of(active, gate_raw, columns):
        return (active * (gate_raw * gate_scale[columns].reshape(1, -1))).astype(BF16)

    def slab(u):
        return w[u].reshape(WIDTH, PAIR)

    def feed_up(j):
        raw[...] = jnp.dot(normed[...], slab(U_FF + 2 * j), preferred_element_type=F32)

    def feed_gate(j):
        columns = block_of(j)
        for s in range(SEQS):
            some = slice(s * LENGTH, (s + 1) * LENGTH)
            raw[some, :] = activation(raw[some, :], columns)
        gate_raw = jnp.dot(normed[...], slab(U_FF + 2 * j + 1), preferred_element_type=F32)
        hid[:, columns] = hidden_of(raw[...], gate_raw, columns)

    def feed_last(_):
        both = jnp.dot(normed[...], slab(U_LAST), preferred_element_type=F32)
        columns = pl.ds(10 * LANES, LANES)
        for s in range(SEQS):
            some = slice(s * LENGTH, (s + 1) * LENGTH)
            active = activation(both[some, :LANES], columns)
            hid[some, columns] = hidden_of(active, both[some, LANES:], columns)

    def down_first(n):
        side, block = n // 4, lax.rem(n, 4)
        right = jnp.concatenate(
            [w[u, side, block].reshape(256, PAIR) for u in range(U_DOWN, U_TILE)], axis=1
        )
        acc[:, block_of(n)] = dot_nt(hid[:, 0:FIRST], right)

    def down_rest(side, block):
        right = jnp.concatenate(
            [w_tile[k, side, block].reshape(256, LANES) for k in range(TILES)], axis=1
        )
        return acc[:, block_of(side * 4 + block)] + dot_nt(hid[:, FIRST:HID], right)

    def compute(m):
        start = 0
        starts = {}
        for name, count in PIECES:
            starts[name] = (start, count)
            start += count

        def during(name, body):
            first_one, count = starts[name]

            @pl.when((m >= first_one) & (m < first_one + count))
            def _():
                body(m - first_one)

        def share(_):
            for load in loads[5:]:
                load.wait()
            across(x_hbm, x.at[tp], X_INPUT).start()
            across(gain_hbm, mate_gain, X_GAIN).start()
            across(out_scale_hbm, mate_out_scale, X_SCALE).start()

        def pooling(s):
            @pl.when(s == 0)
            def _():
                across(x_hbm, x.at[mate], X_INPUT).wait_recv()
                across(gain_hbm, mate_gain, X_GAIN).wait_recv()
                across(out_scale_hbm, mate_out_scale, X_SCALE).wait_recv()

            pool(s)

        def projecting(k):
            side = jnp.where(k < 4, mate, tp)
            block = lax.rem(k, 4)
            project(side, block)
            mixer_piece(side, block).start()

        def norming(s):
            @pl.when(s == 0)
            def _():
                across(part, got, X_MIXER).wait_recv()

            norm(s)

        def feeding(k):
            @pl.when(lax.rem(k, 2) == 0)
            def _():
                feed_up(k // 2)

            @pl.when(lax.rem(k, 2) == 1)
            def _():
                feed_gate(k // 2)

        during("share", share)
        during("pool", pooling)
        during("group", group)
        during("project", projecting)
        during("norm", norming)
        during("last", feed_last)
        again = starts["feed again"][0]
        early, late = (m >= starts["feed"][0]) & (m < starts["down"][0]), m >= again

        @pl.when(early | late)
        def _():
            feeding(jnp.where(late, m - again + starts["feed"][1], m - starts["feed"][0]))

        during("down", down_first)

    def micro(m, _):
        def among(low, high):
            if high - low == 1:
                gather(low)
                return
            half = (low + high) // 2
            pl.when(m < half)(lambda: among(low, half))
            pl.when(m >= half)(lambda: among(half, high))

        among(0, TOTAL)
        compute(m)
        return 0

    lax.fori_loop(0, TOTAL, micro, 0)
    gather(TOTAL)

    across(part, got, X_MIXER).wait_send()

    def first_half(block, _):
        part[mate, :, block_of(block)] = down_rest(mate, block).astype(BF16)
        final_piece(block).start()
        return 0

    lax.fori_loop(0, 4, first_half, 0)

    def second_half(block, _):
        columns = block_of(block)
        final_piece(block).wait_recv()
        total = down_rest(tp, block).astype(BF16).astype(F32) + end[:, columns].astype(F32)
        scale = down_scale[columns].reshape(1, PAIR)
        y[:, columns] = (mid[tp, :, columns].astype(F32) + total * scale).astype(BF16)
        return 0

    lax.fori_loop(0, 4, second_half, 0)

    across(x_hbm, x.at[tp], X_INPUT).wait_send()
    across(gain_hbm, mate_gain, X_GAIN).wait_send()
    across(out_scale_hbm, mate_out_scale, X_SCALE).wait_send()
    for block in range(4):
        final_piece(block).wait_send()
    full, over = divmod(U_TILE, SEND_GROUP)
    lanes = [2 * PAIR * SEND_GROUP] * full + [2 * PAIR * over, PAIR * TILES]
    for k in range(full + 2):
        ref = normed.at[pl.ds(0, 31 * 32), pl.ds(0, lanes[k])]
        pltpu.make_async_copy(ref, ref, send_sem.at[k]).wait()


def layer(
    layer_in,
    mix_gain,
    pool_weight,
    pool_scale,
    out_weight,
    out_scale,
    channel_gain,
    up_weight,
    up_scale,
    gate_weight,
    gate_scale,
    conv_weight,
    down_weight,
    down_scale,
):
    anywhere = pl.BlockSpec(memory_space=pl.ANY)
    dma = pltpu.SemaphoreType.DMA
    return pl.pallas_call(
        kernel,
        out_shape=pltpu.VMEM((ROWS, HALF), BF16),
        in_specs=[anywhere] * 14,
        out_specs=pl.BlockSpec(memory_space=pltpu.VMEM),
        scratch_shapes=[
            pltpu.VMEM((U_TILE, 2, 4, 4, 64, PAIR), BF16),
            pltpu.VMEM((TILES, 2, 4, 4, 64, LANES), BF16),
            pltpu.VMEM((2, ROWS, HALF), BF16),
            pltpu.VMEM((2, ROWS, HALF), BF16),
            pltpu.VMEM((2, ROWS, HALF), BF16),
            pltpu.VMEM((ROWS, HALF), BF16),
            pltpu.VMEM((2, ROWS, HALF), BF16),
            pltpu.VMEM((ROWS, WIDTH), BF16),
            pltpu.VMEM((ROWS, HID), BF16),
            pltpu.VMEM((ROWS, WIDTH), F32),
            pltpu.VMEM((ROWS, PAIR), F32),
            pltpu.VMEM((2, 16, 512), F32),
            pltpu.VMEM((64, HALF), F32),
            pltpu.VMEM((64, HID), F32),
            pltpu.VMEM((64, HID), F32),
            pltpu.VMEM((64, HID), F32),
            pltpu.VMEM((HALF,), BF16),
            pltpu.VMEM((2, 512), F32),
            pltpu.VMEM((HALF,), F32),
            pltpu.VMEM((HALF,), F32),
            pltpu.VMEM((HALF,), BF16),
            pltpu.VMEM((HALF,), BF16),
            pltpu.VMEM((HID,), F32),
            pltpu.VMEM((HID,), F32),
            pltpu.VMEM((3, HID), F32),
            pltpu.VMEM((HALF,), F32),
            dma((14,)),
            dma((group_of(U_TILE) + 1,)),
            dma((UNITS, STAGES)),
            dma((8,)),
            dma((8,)),
        ],
        compiler_params=pltpu.CompilerParams(
            collective_id=0, has_side_effects=True, vmem_limit_bytes=63_500_000
        ),
    )(
        layer_in,
        pool_weight.transpose(0, 2, 1),
        out_weight.T,
        up_weight,
        gate_weight,
        down_weight.T,
        mix_gain,
        pool_scale,
        out_scale,
        channel_gain,
        up_scale,
        gate_scale,
        conv_weight,
        down_scale,
    )


def solution(mesh):
    torus = Mesh(
        mesh.devices.reshape(mesh.shape["rep"], 2, 4, 4, mesh.shape["tp"]),
        ("rep", "fs_0", "fs_1", "fs_2", "tp"),
    )
    in_specs = (
        P(REP_FS, "tp"),
        P("tp"),
        P("tp", None, FS),
        P("tp", None),
        P("tp", FS),
        P("tp"),
        P("tp"),
        P(FS, "tp"),
        P("tp"),
        P(FS, "tp"),
        P("tp"),
        P(None, "tp"),
        P("tp", FS),
        P("tp"),
    )
    out_specs = P(REP_FS, "tp")
    return jax.shard_map(
        layer, mesh=torus, in_specs=in_specs, out_specs=out_specs, check_vma=False
    )
```

```python
import jax
import jax.numpy as jnp
from jax import lax
from jax.experimental import pallas as pl
from jax.experimental.pallas import tpu as pltpu
from jax.sharding import Mesh
from jax.sharding import PartitionSpec as P

LENGTH = 256
FS = ("fs_0", "fs_1", "fs_2")
REP_FS = ("rep", "fs_0", "fs_1", "fs_2")
EPS = 1e-06

F32 = jnp.float32
BF16 = jnp.bfloat16
MESH = pl.DeviceIdType.MESH

ROWS = 1024
HALF = 1024
WIDTH = 2048
HID = 1408
SEQS = ROWS // LENGTH
LANES = 128
PAIR = 2 * LANES

U_POOL = 0
U_OUT = 1
U_LAST = 5
U_FF = 6
U_DOWN = 16
U_TILE = 19
UNITS = 24
TILES = UNITS - U_TILE
STAGES = 5
SEND_GROUP = 4
FIRST = (U_TILE - U_DOWN) * PAIR

ORDERS = (
    "yxz",
    "yzx",
    "xyz",
    "xzy",
    "xzy",
    "yxz",
    "yzx",
    "yxz",
    "xzy",
    "xzy",
    "yxz",
    "xyz",
    "xyz",
    "xyz",
    "xzy",
    "yzx",
    "yzx",
    "yxz",
    "yzx",
    "xzy",
    "yxz",
    "yzx",
    "xyz",
    "zxy",
)

SCHEDULE = (
    (32, 24, 0, 40, 184,),
    (
        16, 56, 64, 48, 72, 136, 152, 8, 112, 128, 96, 1184, 144, 1032, 1000, 33, 176, 1, 1024,
        1040, 25, 41, 1016, 1056, 17, 88, 57, 160, 120, 1064, 1048, 1072, 1136, 65, 73, 104, 49,
        137, 1152, 1008, 1112, 153, 113, 185, 9, 168, 80, 1128, 1096, 1033, 1144, 97, 145, 129, 34,
        1176, 1001, 2, 1025, 1041, 26, 1017, 18, 1057, 1160, 1088,
    ),
    (
        1065, 1120, 66, 1073, 1049, 1137, 42, 1104, 1009, 1153, 121, 1168, 10, 1113, 169, 161, 1080,
        81,
    ),
    (1185, 1145, 1097, 98, 1129, 146, 1034, 138, 50, 1026, 27,),
    (1002, 1018, 130, 1066, 1121, 1169, 1161, 3, 1081, 74, 1010, 89,),
    (
        1042, 43, 170, 1146, 122, 1098, 11, 1050, 114, 19, 1138, 1130, 154, 35, 1003, 4, 1089, 1074,
        1170, 1043, 1122, 1027, 139, 1114, 1019, 186, 1154, 58, 28, 20, 1011, 12, 90, 1139, 1186,
        1035, 1004,
    ),
    (82, 36,),
    (1058, 44, 1028, 59, 75, 51, 1012, 1090, 1020,),
    (),
    (),
    (1082, 140,),
    (1036,),
    (),
    (1059, 91,),
    (),
    (83,),
    (67,),
    (1044, 177, 105,),
    (131, 60,),
    (),
    (1075,),
    (1051,),
    (1091,),
    (1083, 1177, 76, 1105, 1140,),
    (52,),
    (106, 92,),
    (),
    (1067, 147,),
    (1131, 1060, 68, 1076, 84, 99, 1052,),
    (132, 178,),
    (1106, 107, 1092, 162, 115, 1068,),
    (1147, 1099, 148, 100,),
    (1178, 123, 1132, 1107, 1084,),
    (1162, 179, 187, 108,),
    (1148,),
    (155,),
    (163,),
    (1115, 1100, 1179, 171,),
    (),
    (116, 180,),
    (),
    (1187,),
    (1123, 124,),
    (1163, 188, 164, 1108,),
    (1155, 1171, 172, 156, 1180, 1116,),
    (1124,),
    (1188, 1164, 1172, 1156,),
)

PIECES = (
    ("share", 1),
    ("pool", 4),
    ("group", 2),
    ("project half", 8),
    ("project", 8),
    ("norm", 4),
    ("last", 1),
    ("feed", 6),
    ("down", 8),
    ("feed again", 4),
)
TOTAL = sum(count for _, count in PIECES)

AXIS = {"x": "fs_2", "y": "fs_1"}
GELU_A = 0.7978845608028654
GELU_B = 0.044715

X_GAIN, X_SCALE, X_INPUT, X_MIXER, X_FINAL = 0, 1, 2, 3, 4


def steps_of(order):
    steps = []
    for phase, dim in enumerate(order):
        steps += [(phase, "a")] if dim == "z" else [(phase, "a"), (phase, "b")]
    return steps


def shards_in(order, stage):
    phase, step = steps_of(order)[stage]
    held = 1
    for dim in order[:phase]:
        held *= 2 if dim == "z" else 4
    return held if order[phase] == "z" or step == "b" else 2 * held


def group_of(u):
    return -(-U_TILE // SEND_GROUP) if u >= U_TILE else u // SEND_GROUP


def dot_nt(left, right):
    return lax.dot_general(left, right, (((1,), (1,)), ((), ())), preferred_element_type=F32)


def kernel(
    x_hbm,
    pool_hbm,
    out_hbm,
    up_hbm,
    gate_hbm,
    down_hbm,
    mix_gain_hbm,
    pool_scale_hbm,
    out_scale_hbm,
    gain_hbm,
    up_scale_hbm,
    gate_scale_hbm,
    conv_hbm,
    down_scale_hbm,
    y,
    w,
    w_tile,
    x,
    part,
    got,
    end,
    mid,
    normed,
    hid,
    acc,
    raw,
    st_pool,
    st_out,
    st_up,
    st_gate,
    st_down,
    mix_gain,
    pool_scale,
    out_scale,
    mate_out_scale,
    gain,
    mate_gain,
    up_scale,
    gate_scale,
    conv_taps,
    down_scale,
    in_sem,
    send_sem,
    recv_sem,
    tp_send,
    tp_recv,
):
    rep = lax.axis_index("rep")
    zl = lax.axis_index("fs_0")
    me = {"z": zl, "y": lax.axis_index("fs_1"), "x": lax.axis_index("fs_2")}
    tp = lax.axis_index("tp")
    mate = 1 - tp
    zz = rep * 2 + zl
    z_up = lax.rem(zz + 1, 4)
    z_down = lax.rem(zz + 3, 4)

    def to_z(place):
        return {"rep": place // 2, "fs_0": lax.rem(place, 2)}

    def ring(dim, shift):
        return lax.rem(me[dim] + shift + 4, 4)

    peers = [to_z(z_up), to_z(z_down), {"tp": mate}]
    for dim in ("x", "y"):
        peers += [{AXIS[dim]: ring(dim, 1)}, {AXIS[dim]: ring(dim, -1)}]

    barrier = pltpu.get_barrier_semaphore()
    for peer in peers:
        pl.semaphore_signal(barrier, inc=1, device_id=peer, device_id_type=MESH)

    loads = [
        pltpu.make_async_copy(src, dst, in_sem.at[k])
        for k, (src, dst) in enumerate(
            (
                (pool_hbm, st_pool),
                (out_hbm, st_out),
                (up_hbm, st_up),
                (gate_hbm, st_gate),
                (down_hbm, st_down),
                (x_hbm, x.at[tp]),
                (mix_gain_hbm, mix_gain),
                (pool_scale_hbm, pool_scale),
                (out_scale_hbm, out_scale),
                (gain_hbm, gain),
                (up_scale_hbm, up_scale),
                (gate_scale_hbm, gate_scale),
                (conv_hbm, conv_taps),
                (down_scale_hbm, down_scale),
            )
        )
    ]
    for load in loads[:5]:
        load.start()
    for load in loads[:5]:
        load.wait()

    mine = (me["z"], me["y"], me["x"])
    for g in range(2):
        for ct in range(4):
            block = st_pool[g, :, ct * LANES : (ct + 1) * LANES]
            lanes = pl.ds(g * LANES, LANES)
            w[(U_POOL, *mine, pl.ds(ct * 16, 16), lanes)] = block.astype(BF16)
    for k in range(4):
        w[(U_OUT + k, *mine)] = st_out[:, k * PAIR : (k + 1) * PAIR].astype(BF16)
    for k in range(5):
        columns = slice(k * PAIR, (k + 1) * PAIR)
        w[(U_FF + 2 * k, *mine)] = st_up[:, columns].astype(BF16)
        w[(U_FF + 2 * k + 1, *mine)] = st_gate[:, columns].astype(BF16)
    rest = slice(10 * LANES, HID)
    w[(U_LAST, *mine, slice(None), pl.ds(0, LANES))] = st_up[:, rest].astype(BF16)
    w[(U_LAST, *mine, slice(None), pl.ds(LANES, LANES))] = st_gate[:, rest].astype(BF16)
    for k in range(U_TILE - U_DOWN):
        w[(U_DOWN + k, *mine)] = st_down[:, k * PAIR : (k + 1) * PAIR].astype(BF16)
    for k in range(TILES):
        columns = slice(FIRST + k * LANES, FIRST + (k + 1) * LANES)
        w_tile[(k, *mine)] = st_down[:, columns].astype(BF16)
    for load in loads[5:]:
        load.start()

    pl.semaphore_wait(barrier, len(peers))

    def across(src, dst, index):
        return pltpu.make_async_remote_copy(
            src_ref=src,
            dst_ref=dst,
            send_sem=tp_send.at[index],
            recv_sem=tp_recv.at[index],
            device_id={"tp": mate},
            device_id_type=MESH,
        )

    def region(u, order, phase, place, rows):
        picks = {}
        for k, dim in enumerate(order):
            if k < phase:
                picks[dim] = slice(None)
            elif k == phase:
                picks[dim] = pl.ds(place, 1)
            else:
                picks[dim] = pl.ds(me[dim], 1)
        where = (picks["z"], picks["y"], picks["x"], rows, slice(None))
        return w_tile.at[(u - U_TILE, *where)] if u >= U_TILE else w.at[(u, *where)]

    every, first, second = pl.ds(0, 64), pl.ds(0, 32), pl.ds(32, 32)

    def moves(u, stage):
        order = ORDERS[u]
        phase, step = steps_of(order)[stage]
        dim = order[phase]
        if dim == "z":
            return phase, ((zl, first, to_z(z_up)), (zl, second, to_z(z_down)))
        right, left = {AXIS[dim]: ring(dim, 1)}, {AXIS[dim]: ring(dim, -1)}
        if step == "a":
            return phase, ((me[dim], every, right), (me[dim], every, left))
        return phase, ((ring(dim, -1), first, right), (ring(dim, 1), second, left))

    def send(u, stage):
        phase, both = moves(u, stage)
        for place, rows, peer in both:
            ref = region(u, ORDERS[u], phase, place, rows)
            pltpu.make_async_remote_copy(
                src_ref=ref,
                dst_ref=ref,
                send_sem=send_sem.at[group_of(u)],
                recv_sem=recv_sem.at[u, stage],
                device_id=peer,
                device_id_type=MESH,
            ).start()

    def arrived(u, stage):
        count = shards_in(ORDERS[u], stage)
        box = {1: (1, 1, 1), 2: (1, 1, 2), 4: (1, 1, 4), 8: (1, 2, 4), 16: (1, 4, 4)}[count]
        where = tuple(pl.ds(0, size) for size in box)
        ref = w_tile.at[(u - U_TILE, *where)] if u >= U_TILE else w.at[(u, *where)]
        pltpu.make_async_copy(ref, ref, recv_sem.at[u, stage]).wait()

    def gather(position):
        for code in SCHEDULE[position]:
            u, stage = divmod(code % 1000, 8)
            (arrived if code >= 1000 else send)(u, stage)

    def row(ref):
        return ref[...].astype(F32).reshape(1, ref.shape[0])

    def rows_of(s):
        return pl.ds(pl.multiple_of(s * LENGTH, LENGTH), LENGTH)

    def block_of(n):
        return pl.ds(pl.multiple_of(n * PAIR, PAIR), PAIR)

    mixed = hid

    def pool(s):
        total = jnp.zeros((LENGTH, 1), F32)
        for side in range(2):
            values = x[side, rows_of(s), :].astype(F32)
            total = total + jnp.sum(values * values, axis=1, keepdims=True)
        scale = lax.rsqrt(total / WIDTH + EPS)
        at = lax.broadcasted_iota(jnp.int32, (LENGTH, LENGTH), 0)
        col = lax.broadcasted_iota(jnp.int32, (LENGTH, LENGTH), 1)
        for g in range(2):
            reach = jnp.where(tp == 0, 1 << g, 4 << g)
            lower = jnp.maximum(at - reach, 0)
            upper = jnp.minimum(at + reach, LENGTH)
            band = jnp.where((col >= lower) & (col < upper), 1.0, 0.0).astype(BF16)
            count = (upper[:, :1] - lower[:, :1]).astype(F32)
            columns = slice(g * 512, (g + 1) * 512)
            piece = x[tp, rows_of(s), columns].astype(F32) * scale * row(mix_gain)[:, columns]
            piece = piece.astype(BF16)
            window = jnp.dot(band, piece, preferred_element_type=F32)
            mixed[rows_of(s), columns] = (window / count - piece.astype(F32)).astype(BF16)

    def group(g):
        columns = pl.ds(pl.multiple_of(g * 512, 512), 512)
        lanes = pl.ds(pl.multiple_of(g * LANES, LANES), LANES)
        maps = w[U_POOL, :, :, :, :, lanes].reshape(32, 4, 16, LANES)
        right = jnp.concatenate([maps[:, ct].reshape(512, LANES) for ct in range(4)], axis=1)
        out = dot_nt(mixed[:, columns], right) * pool_scale[pl.ds(g, 1), :]
        normed[:, columns] = out.astype(BF16)

    def project(side, block, units, columns):
        right = jnp.concatenate([w[u, side, block].reshape(256, PAIR) for u in units], axis=1)
        return dot_nt(normed[:, columns], right)

    def sides(k):
        return jnp.where(k < 4, mate, tp), lax.rem(k, 4)

    def project_half(k):
        side, block = sides(k)
        acc[:, block_of(k)] = project(side, block, range(U_OUT, U_OUT + 2), slice(0, 512))

    def project_rest(k):
        side, block = sides(k)
        rest = project(side, block, range(U_OUT + 2, U_OUT + 4), slice(512, HALF))
        part[side, :, block_of(block)] = (acc[:, block_of(k)] + rest).astype(BF16)
        mixer_piece(side, block).start()

    def mixer_piece(side, block):
        columns = block_of(block)
        return across(part.at[side, :, columns], got.at[side, :, columns], X_MIXER)

    def final_piece(block):
        columns = block_of(block)
        return across(part.at[mate, :, columns], end.at[:, columns], X_FINAL + block)

    def norm(s):
        ours, theirs = row(gain), row(mate_gain)
        gains = (jnp.where(tp == 0, ours, theirs), jnp.where(tp == 0, theirs, ours))
        ours, theirs = row(out_scale), row(mate_out_scale)
        scales = (jnp.where(tp == 0, ours, theirs), jnp.where(tp == 0, theirs, ours))
        total = jnp.zeros((LENGTH, 1), F32)
        for side in range(2):
            added = part[side, rows_of(s), :].astype(F32) + got[side, rows_of(s), :].astype(F32)
            value = x[side, rows_of(s), :].astype(F32) + added * scales[side]
            value = value.astype(BF16)
            mid[side, rows_of(s), :] = value
            value = value.astype(F32)
            total = total + jnp.sum(value * value, axis=1, keepdims=True)
        scale = lax.rsqrt(total / WIDTH + EPS)
        for side in range(2):
            value = mid[side, rows_of(s), :].astype(F32) * scale * gains[side]
            normed[rows_of(s), side * HALF : (side + 1) * HALF] = value.astype(BF16)

    def activation(up_raw, columns):
        taps = conv_taps[:, columns]
        ups = up_scale[columns].reshape(1, -1)
        lifted = (up_raw * ups).astype(BF16).astype(F32)
        at = lax.broadcasted_iota(jnp.int32, lifted.shape, 0)
        before = jnp.where(at == 0, 0.0, pltpu.roll(lifted, 1, 0))
        after = jnp.where(at == LENGTH - 1, 0.0, pltpu.roll(lifted, LENGTH - 1, 0))
        conv = taps[0:1] * before + taps[1:2] * lifted + taps[2:3] * after
        inner = conv * (GELU_A + (GELU_A * GELU_B) * (conv * conv))
        return conv + conv * jnp.tanh(inner)

    def hidden_of(active, gate_raw, columns):
        half_scale = 0.5 * gate_scale[columns].reshape(1, -1)
        return (active * (gate_raw * half_scale)).astype(BF16)

    def slab(u):
        return w[u].reshape(WIDTH, PAIR)

    def feed_up(j):
        raw[...] = jnp.dot(normed[...], slab(U_FF + 2 * j), preferred_element_type=F32)

    def feed_gate(j):
        columns = block_of(j)
        for s in range(SEQS):
            some = slice(s * LENGTH, (s + 1) * LENGTH)
            raw[some, :] = activation(raw[some, :], columns)
        gate_raw = jnp.dot(normed[...], slab(U_FF + 2 * j + 1), preferred_element_type=F32)
        hid[:, columns] = hidden_of(raw[...], gate_raw, columns)

    def feed_last(_):
        both = jnp.dot(normed[...], slab(U_LAST), preferred_element_type=F32)
        columns = pl.ds(10 * LANES, LANES)
        for s in range(SEQS):
            some = slice(s * LENGTH, (s + 1) * LENGTH)
            active = activation(both[some, :LANES], columns)
            hid[some, columns] = hidden_of(active, both[some, LANES:], columns)

    def down_first(n):
        side, block = n // 4, lax.rem(n, 4)
        right = jnp.concatenate(
            [w[u, side, block].reshape(256, PAIR) for u in range(U_DOWN, U_TILE)], axis=1
        )
        acc[:, block_of(n)] = dot_nt(hid[:, 0:FIRST], right)

    def down_rest(side, block):
        right = jnp.concatenate(
            [w_tile[k, side, block].reshape(256, LANES) for k in range(TILES)], axis=1
        )
        return acc[:, block_of(side * 4 + block)] + dot_nt(hid[:, FIRST:HID], right)

    def compute(m):
        start = 0
        starts = {}
        for name, count in PIECES:
            starts[name] = (start, count)
            start += count

        def during(name, body):
            first_one, count = starts[name]

            @pl.when((m >= first_one) & (m < first_one + count))
            def _():
                body(m - first_one)

        def share(_):
            for load in loads[5:]:
                load.wait()
            across(x_hbm, x.at[tp], X_INPUT).start()
            across(gain_hbm, mate_gain, X_GAIN).start()
            across(out_scale_hbm, mate_out_scale, X_SCALE).start()

        def pooling(s):
            @pl.when(s == 0)
            def _():
                across(x_hbm, x.at[mate], X_INPUT).wait_recv()
                across(gain_hbm, mate_gain, X_GAIN).wait_recv()
                across(out_scale_hbm, mate_out_scale, X_SCALE).wait_recv()

            pool(s)

        def norming(s):
            @pl.when(s == 0)
            def _():
                across(part, got, X_MIXER).wait_recv()

            norm(s)

        def feeding(k):
            @pl.when(lax.rem(k, 2) == 0)
            def _():
                feed_up(k // 2)

            @pl.when(lax.rem(k, 2) == 1)
            def _():
                feed_gate(k // 2)

        during("share", share)
        during("pool", pooling)
        during("group", group)
        during("project half", project_half)
        during("project", project_rest)
        during("norm", norming)
        during("last", feed_last)
        again = starts["feed again"][0]
        early, late = (m >= starts["feed"][0]) & (m < starts["down"][0]), m >= again

        @pl.when(early | late)
        def _():
            feeding(jnp.where(late, m - again + starts["feed"][1], m - starts["feed"][0]))

        during("down", down_first)

    def micro(m, _):
        def among(low, high):
            if high - low == 1:
                gather(low)
                return
            half = (low + high) // 2
            pl.when(m < half)(lambda: among(low, half))
            pl.when(m >= half)(lambda: among(half, high))

        among(0, TOTAL)
        compute(m)
        return 0

    lax.fori_loop(0, TOTAL, micro, 0)
    gather(TOTAL)

    across(part, got, X_MIXER).wait_send()

    def first_half(block, _):
        part[mate, :, block_of(block)] = down_rest(mate, block).astype(BF16)
        final_piece(block).start()
        return 0

    lax.fori_loop(0, 4, first_half, 0)

    def second_half(block, _):
        columns = block_of(block)
        final_piece(block).wait_recv()
        total = down_rest(tp, block).astype(BF16).astype(F32) + end[:, columns].astype(F32)
        scale = down_scale[columns].reshape(1, PAIR)
        y[:, columns] = (mid[tp, :, columns].astype(F32) + total * scale).astype(BF16)
        return 0

    lax.fori_loop(0, 4, second_half, 0)

    across(x_hbm, x.at[tp], X_INPUT).wait_send()
    across(gain_hbm, mate_gain, X_GAIN).wait_send()
    across(out_scale_hbm, mate_out_scale, X_SCALE).wait_send()
    for block in range(4):
        final_piece(block).wait_send()
    full, over = divmod(U_TILE, SEND_GROUP)
    lanes = [2 * PAIR * SEND_GROUP] * full + [2 * PAIR * over, PAIR * TILES]
    for k in range(full + 2):
        ref = normed.at[pl.ds(0, 31 * 32), pl.ds(0, lanes[k])]
        pltpu.make_async_copy(ref, ref, send_sem.at[k]).wait()


def layer(
    layer_in,
    mix_gain,
    pool_weight,
    pool_scale,
    out_weight,
    out_scale,
    channel_gain,
    up_weight,
    up_scale,
    gate_weight,
    gate_scale,
    conv_weight,
    down_weight,
    down_scale,
):
    anywhere = pl.BlockSpec(memory_space=pl.ANY)
    dma = pltpu.SemaphoreType.DMA
    return pl.pallas_call(
        kernel,
        out_shape=pltpu.VMEM((ROWS, HALF), BF16),
        in_specs=[anywhere] * 14,
        out_specs=pl.BlockSpec(memory_space=pltpu.VMEM),
        scratch_shapes=[
            pltpu.VMEM((U_TILE, 2, 4, 4, 64, PAIR), BF16),
            pltpu.VMEM((TILES, 2, 4, 4, 64, LANES), BF16),
            pltpu.VMEM((2, ROWS, HALF), BF16),
            pltpu.VMEM((2, ROWS, HALF), BF16),
            pltpu.VMEM((2, ROWS, HALF), BF16),
            pltpu.VMEM((ROWS, HALF), BF16),
            pltpu.VMEM((2, ROWS, HALF), BF16),
            pltpu.VMEM((ROWS, WIDTH), BF16),
            pltpu.VMEM((ROWS, HID), BF16),
            pltpu.VMEM((ROWS, WIDTH), F32),
            pltpu.VMEM((ROWS, PAIR), F32),
            pltpu.VMEM((2, 16, 512), F32),
            pltpu.VMEM((64, HALF), F32),
            pltpu.VMEM((64, HID), F32),
            pltpu.VMEM((64, HID), F32),
            pltpu.VMEM((64, HID), F32),
            pltpu.VMEM((HALF,), BF16),
            pltpu.VMEM((2, 512), F32),
            pltpu.VMEM((HALF,), F32),
            pltpu.VMEM((HALF,), F32),
            pltpu.VMEM((HALF,), BF16),
            pltpu.VMEM((HALF,), BF16),
            pltpu.VMEM((HID,), F32),
            pltpu.VMEM((HID,), F32),
            pltpu.VMEM((3, HID), F32),
            pltpu.VMEM((HALF,), F32),
            dma((14,)),
            dma((group_of(U_TILE) + 1,)),
            dma((UNITS, STAGES)),
            dma((8,)),
            dma((8,)),
        ],
        compiler_params=pltpu.CompilerParams(
            collective_id=0, has_side_effects=True, vmem_limit_bytes=63_500_000
        ),
    )(
        layer_in,
        pool_weight.transpose(0, 2, 1),
        out_weight.T,
        up_weight,
        gate_weight,
        down_weight.T,
        mix_gain,
        pool_scale,
        out_scale,
        channel_gain,
        up_scale,
        gate_scale,
        conv_weight,
        down_scale,
    )


def solution(mesh):
    torus = Mesh(
        mesh.devices.reshape(mesh.shape["rep"], 2, 4, 4, mesh.shape["tp"]),
        ("rep", "fs_0", "fs_1", "fs_2", "tp"),
    )
    in_specs = (
        P(REP_FS, "tp"),
        P("tp"),
        P("tp", None, FS),
        P("tp", None),
        P("tp", FS),
        P("tp"),
        P("tp"),
        P(FS, "tp"),
        P("tp"),
        P(FS, "tp"),
        P("tp"),
        P(None, "tp"),
        P("tp", FS),
        P("tp"),
    )
    out_specs = P(REP_FS, "tp")
    return jax.shard_map(
        layer, mesh=torus, in_specs=in_specs, out_specs=out_specs, check_vma=False
    )
```

```python
import jax
import jax.numpy as jnp
from jax import lax
from jax.experimental import pallas as pl
from jax.experimental.pallas import tpu as pltpu
from jax.sharding import Mesh
from jax.sharding import PartitionSpec as P

LENGTH = 256
FS = ("fs_0", "fs_1", "fs_2")
REP_FS = ("rep", "fs_0", "fs_1", "fs_2")
EPS = 1e-06

F32 = jnp.float32
BF16 = jnp.bfloat16
MESH = pl.DeviceIdType.MESH

ROWS = 1024
HALF = 1024
WIDTH = 2048
HID = 1408
SEQS = ROWS // LENGTH
LANES = 128
PAIR = 2 * LANES

U_POOL = 0
U_OUT = 1
U_LAST = 5
U_FF = 6
U_DOWN = 16
U_TILE = 19
UNITS = 24
TILES = UNITS - U_TILE
STAGES = 5
SEND_GROUP = 4
FIRST = (U_TILE - U_DOWN) * PAIR

ORDERS = (
    "yxz",
    "yzx",
    "xyz",
    "xzy",
    "xzy",
    "yxz",
    "yzx",
    "yxz",
    "xzy",
    "xzy",
    "yxz",
    "xyz",
    "xyz",
    "xyz",
    "xzy",
    "yzx",
    "yzx",
    "yxz",
    "yzx",
    "xzy",
    "yxz",
    "yzx",
    "xyz",
    "zxy",
)

SCHEDULE = (
    (32, 24, 0, 40, 184,),
    (
        16, 56, 64, 48, 72, 136, 152, 8, 112, 128, 96, 1184, 144, 1032, 1000, 33, 176, 1, 1024,
        1040, 25, 41, 1016, 1056, 17, 88, 57, 160, 120, 1064, 1048, 1072, 1136, 65, 73, 104, 49,
        137, 1152, 1008, 1112, 153, 113, 185, 9, 168, 80, 1128, 1096, 1033, 1144, 97, 145, 129, 34,
        1176, 1001, 2, 1025, 1041, 26, 1017, 18, 1057, 1160, 1088,
    ),
    (
        1065, 1120, 66, 1073, 1049, 1137, 42, 1104, 1009, 1153, 121, 1168, 10, 1113, 169, 161, 1080,
        81,
    ),
    (1185, 1145, 1097, 98, 1129, 146, 1034, 138, 50, 1026, 27,),
    (1002, 1018, 130, 1066, 1121, 1169, 1161, 3, 1081, 74, 1010, 89,),
    (
        1042, 43, 170, 1146, 122, 1098, 11, 1050, 114, 19, 1138, 1130, 154, 35, 1003, 4, 1089, 1074,
        1170, 1043, 1122, 1027, 139, 1114, 1019, 186, 1154, 58, 28, 20, 1011, 12, 90, 1139, 1186,
        1035, 1004,
    ),
    (82, 36,),
    (1058, 44, 1028, 59, 75, 51, 1012, 1090, 1020,),
    (),
    (),
    (1082, 140,),
    (1036,),
    (),
    (1059, 91,),
    (),
    (83,),
    (67,),
    (1044, 177, 105,),
    (131, 60,),
    (),
    (1075,),
    (1051,),
    (1091,),
    (1083, 1177, 76, 1105, 1140,),
    (52,),
    (106, 92,),
    (),
    (1067, 147,),
    (1131, 1060, 68, 1076, 84, 99, 1052,),
    (132, 178,),
    (1106, 107, 1092, 162, 115, 1068,),
    (1147, 1099, 148, 100,),
    (1178, 123, 1132, 1107, 1084,),
    (1162, 179, 187, 108,),
    (1148,),
    (155,),
    (163,),
    (1115, 1100, 1179, 171,),
    (),
    (116, 180,),
    (),
    (1187,),
    (1123, 124,),
    (1163, 188, 164, 1108,),
    (1155, 1171, 172, 156, 1180, 1116,),
    (1124,),
    (1188, 1164, 1172, 1156,),
)

PIECES = (
    ("share", 1),
    ("pool", 4),
    ("group", 2),
    ("project half", 8),
    ("project", 8),
    ("norm", 4),
    ("last", 1),
    ("feed", 6),
    ("down", 8),
    ("feed again", 4),
)
TOTAL = sum(count for _, count in PIECES)

AXIS = {"x": "fs_2", "y": "fs_1"}
GELU_A = 0.7978845608028654
GELU_B = 0.044715

X_GAIN, X_SCALE, X_INPUT, X_MIXER, X_FINAL = 0, 1, 2, 3, 4


def steps_of(order):
    steps = []
    for phase, dim in enumerate(order):
        steps += [(phase, "a")] if dim == "z" else [(phase, "a"), (phase, "b")]
    return steps


def shards_in(order, stage):
    phase, step = steps_of(order)[stage]
    held = 1
    for dim in order[:phase]:
        held *= 2 if dim == "z" else 4
    return held if order[phase] == "z" or step == "b" else 2 * held


def group_of(u):
    return -(-U_TILE // SEND_GROUP) if u >= U_TILE else u // SEND_GROUP


def dot_nt(left, right):
    return lax.dot_general(left, right, (((1,), (1,)), ((), ())), preferred_element_type=F32)


def kernel(
    x_hbm,
    pool_hbm,
    out_hbm,
    up_hbm,
    gate_hbm,
    down_hbm,
    mix_gain_hbm,
    pool_scale_hbm,
    out_scale_hbm,
    gain_hbm,
    up_scale_hbm,
    gate_scale_hbm,
    conv_hbm,
    down_scale_hbm,
    y,
    w,
    w_tile,
    x,
    part,
    got,
    end,
    mid,
    normed,
    hid,
    acc,
    raw,
    st_pool,
    st_out,
    st_up,
    st_gate,
    st_down,
    mix_gain,
    pool_scale,
    out_scale,
    mate_out_scale,
    gain,
    mate_gain,
    up_scale,
    gate_scale,
    conv_taps,
    down_scale,
    in_sem,
    send_sem,
    recv_sem,
    tp_send,
    tp_recv,
):
    rep = lax.axis_index("rep")
    zl = lax.axis_index("fs_0")
    me = {"z": zl, "y": lax.axis_index("fs_1"), "x": lax.axis_index("fs_2")}
    tp = lax.axis_index("tp")
    mate = 1 - tp
    zz = rep * 2 + zl
    z_up = lax.rem(zz + 1, 4)
    z_down = lax.rem(zz + 3, 4)

    def to_z(place):
        return {"rep": place // 2, "fs_0": lax.rem(place, 2)}

    def ring(dim, shift):
        return lax.rem(me[dim] + shift + 4, 4)

    peers = [to_z(z_up), to_z(z_down), {"tp": mate}]
    for dim in ("x", "y"):
        peers += [{AXIS[dim]: ring(dim, 1)}, {AXIS[dim]: ring(dim, -1)}]

    barrier = pltpu.get_barrier_semaphore()
    for peer in peers:
        pl.semaphore_signal(barrier, inc=1, device_id=peer, device_id_type=MESH)

    loads = [
        pltpu.make_async_copy(src, dst, in_sem.at[k])
        for k, (src, dst) in enumerate(
            (
                (pool_hbm, st_pool),
                (out_hbm, st_out),
                (up_hbm, st_up),
                (gate_hbm, st_gate),
                (down_hbm, st_down),
                (x_hbm, x.at[tp]),
                (mix_gain_hbm, mix_gain),
                (pool_scale_hbm, pool_scale),
                (out_scale_hbm, out_scale),
                (gain_hbm, gain),
                (up_scale_hbm, up_scale),
                (gate_scale_hbm, gate_scale),
                (conv_hbm, conv_taps),
                (down_scale_hbm, down_scale),
            )
        )
    ]
    for load in loads[:5]:
        load.start()
    for load in loads[:5]:
        load.wait()

    mine = (me["z"], me["y"], me["x"])
    for g in range(2):
        for ct in range(4):
            block = st_pool[g, :, ct * LANES : (ct + 1) * LANES]
            lanes = pl.ds(g * LANES, LANES)
            w[(U_POOL, *mine, pl.ds(ct * 16, 16), lanes)] = block.astype(BF16)
    for k in range(4):
        w[(U_OUT + k, *mine)] = st_out[:, k * PAIR : (k + 1) * PAIR].astype(BF16)
    for k in range(5):
        columns = slice(k * PAIR, (k + 1) * PAIR)
        w[(U_FF + 2 * k, *mine)] = st_up[:, columns].astype(BF16)
        w[(U_FF + 2 * k + 1, *mine)] = st_gate[:, columns].astype(BF16)
    rest = slice(10 * LANES, HID)
    w[(U_LAST, *mine, slice(None), pl.ds(0, LANES))] = st_up[:, rest].astype(BF16)
    w[(U_LAST, *mine, slice(None), pl.ds(LANES, LANES))] = st_gate[:, rest].astype(BF16)
    for k in range(U_TILE - U_DOWN):
        w[(U_DOWN + k, *mine)] = st_down[:, k * PAIR : (k + 1) * PAIR].astype(BF16)
    for k in range(TILES):
        columns = slice(FIRST + k * LANES, FIRST + (k + 1) * LANES)
        w_tile[(k, *mine)] = st_down[:, columns].astype(BF16)
    for load in loads[5:]:
        load.start()

    pl.semaphore_wait(barrier, len(peers))

    def across(src, dst, index):
        return pltpu.make_async_remote_copy(
            src_ref=src,
            dst_ref=dst,
            send_sem=tp_send.at[index],
            recv_sem=tp_recv.at[index],
            device_id={"tp": mate},
            device_id_type=MESH,
        )

    def region(u, order, phase, place, rows):
        picks = {}
        for k, dim in enumerate(order):
            if k < phase:
                picks[dim] = slice(None)
            elif k == phase:
                picks[dim] = pl.ds(place, 1)
            else:
                picks[dim] = pl.ds(me[dim], 1)
        where = (picks["z"], picks["y"], picks["x"], rows, slice(None))
        return w_tile.at[(u - U_TILE, *where)] if u >= U_TILE else w.at[(u, *where)]

    every, first, second = pl.ds(0, 64), pl.ds(0, 32), pl.ds(32, 32)

    def moves(u, stage):
        order = ORDERS[u]
        phase, step = steps_of(order)[stage]
        dim = order[phase]
        if dim == "z":
            return phase, ((zl, first, to_z(z_up)), (zl, second, to_z(z_down)))
        right, left = {AXIS[dim]: ring(dim, 1)}, {AXIS[dim]: ring(dim, -1)}
        if step == "a":
            return phase, ((me[dim], every, right), (me[dim], every, left))
        return phase, ((ring(dim, -1), first, right), (ring(dim, 1), second, left))

    def send(u, stage):
        phase, both = moves(u, stage)
        for place, rows, peer in both:
            ref = region(u, ORDERS[u], phase, place, rows)
            pltpu.make_async_remote_copy(
                src_ref=ref,
                dst_ref=ref,
                send_sem=send_sem.at[group_of(u)],
                recv_sem=recv_sem.at[u, stage],
                device_id=peer,
                device_id_type=MESH,
            ).start()

    def arrived(u, stage):
        count = shards_in(ORDERS[u], stage)
        box = {1: (1, 1, 1), 2: (1, 1, 2), 4: (1, 1, 4), 8: (1, 2, 4), 16: (1, 4, 4)}[count]
        where = tuple(pl.ds(0, size) for size in box)
        ref = w_tile.at[(u - U_TILE, *where)] if u >= U_TILE else w.at[(u, *where)]
        pltpu.make_async_copy(ref, ref, recv_sem.at[u, stage]).wait()

    def gather(position):
        for code in SCHEDULE[position]:
            u, stage = divmod(code % 1000, 8)
            (arrived if code >= 1000 else send)(u, stage)

    def row(ref):
        return ref[...].astype(F32).reshape(1, ref.shape[0])

    def rows_of(s):
        return pl.ds(pl.multiple_of(s * LENGTH, LENGTH), LENGTH)

    def block_of(n):
        return pl.ds(pl.multiple_of(n * PAIR, PAIR), PAIR)

    mixed = hid

    def pool(s):
        total = jnp.zeros((LENGTH, 1), F32)
        for side in range(2):
            values = x[side, rows_of(s), :].astype(F32)
            total = total + jnp.sum(values * values, axis=1, keepdims=True)
        scale = lax.rsqrt(total / WIDTH + EPS)
        at = lax.broadcasted_iota(jnp.int32, (LENGTH, LENGTH), 0)
        col = lax.broadcasted_iota(jnp.int32, (LENGTH, LENGTH), 1)
        for g in range(2):
            reach = jnp.where(tp == 0, 1 << g, 4 << g)
            lower = jnp.maximum(at - reach, 0)
            upper = jnp.minimum(at + reach, LENGTH)
            band = jnp.where((col >= lower) & (col < upper), 1.0, 0.0).astype(BF16)
            count = (upper[:, :1] - lower[:, :1]).astype(F32)
            columns = slice(g * 512, (g + 1) * 512)
            piece = x[tp, rows_of(s), columns].astype(F32) * scale * row(mix_gain)[:, columns]
            piece = piece.astype(BF16)
            window = jnp.dot(band, piece, preferred_element_type=F32)
            mixed[rows_of(s), columns] = (window / count - piece.astype(F32)).astype(BF16)

    def group(g):
        columns = pl.ds(pl.multiple_of(g * 512, 512), 512)
        lanes = pl.ds(pl.multiple_of(g * LANES, LANES), LANES)
        maps = w[U_POOL, :, :, :, :, lanes].reshape(32, 4, 16, LANES)
        right = jnp.concatenate([maps[:, ct].reshape(512, LANES) for ct in range(4)], axis=1)
        out = dot_nt(mixed[:, columns], right) * pool_scale[pl.ds(g, 1), :]
        normed[:, columns] = out.astype(BF16)

    def project(side, block, units, columns):
        right = jnp.concatenate([w[u, side, block].reshape(256, PAIR) for u in units], axis=1)
        return dot_nt(normed[:, columns], right)

    def sides(k):
        return jnp.where(k < 4, mate, tp), lax.rem(k, 4)

    def project_half(k):
        side, block = sides(k)
        acc[:, block_of(k)] = project(side, block, range(U_OUT, U_OUT + 2), slice(0, 512))

    def project_rest(k):
        side, block = sides(k)
        rest = project(side, block, range(U_OUT + 2, U_OUT + 4), slice(512, HALF))
        part[side, :, block_of(block)] = (acc[:, block_of(k)] + rest).astype(BF16)
        mixer_piece(side, block).start()

    def mixer_piece(side, block):
        columns = block_of(block)
        return across(part.at[side, :, columns], got.at[side, :, columns], X_MIXER)

    def final_piece(block):
        columns = block_of(block)
        return across(part.at[mate, :, columns], end.at[:, columns], X_FINAL + block)

    def norm(s):
        ours, theirs = row(gain), row(mate_gain)
        gains = (jnp.where(tp == 0, ours, theirs), jnp.where(tp == 0, theirs, ours))
        ours, theirs = row(out_scale), row(mate_out_scale)
        scales = (jnp.where(tp == 0, ours, theirs), jnp.where(tp == 0, theirs, ours))
        total = jnp.zeros((LENGTH, 1), F32)
        for side in range(2):
            added = part[side, rows_of(s), :].astype(F32) + got[side, rows_of(s), :].astype(F32)
            value = x[side, rows_of(s), :].astype(F32) + added * scales[side]
            value = value.astype(BF16)
            mid[side, rows_of(s), :] = value
            value = value.astype(F32)
            total = total + jnp.sum(value * value, axis=1, keepdims=True)
        scale = lax.rsqrt(total / WIDTH + EPS)
        for side in range(2):
            value = mid[side, rows_of(s), :].astype(F32) * scale * gains[side]
            normed[rows_of(s), side * HALF : (side + 1) * HALF] = value.astype(BF16)

    def activation(up_raw, columns):
        taps = conv_taps[:, columns]
        ups = up_scale[columns].reshape(1, -1)
        lifted = (up_raw * ups).astype(BF16).astype(F32)
        at = lax.broadcasted_iota(jnp.int32, lifted.shape, 0)
        before = jnp.where(at == 0, 0.0, pltpu.roll(lifted, 1, 0))
        after = jnp.where(at == LENGTH - 1, 0.0, pltpu.roll(lifted, LENGTH - 1, 0))
        conv = taps[0:1] * before + taps[1:2] * lifted + taps[2:3] * after
        inner = conv * (GELU_A + (GELU_A * GELU_B) * (conv * conv))
        return conv + conv * jnp.tanh(inner)

    def hidden_of(active, gate_raw, columns):
        half_scale = 0.5 * gate_scale[columns].reshape(1, -1)
        return (active * (gate_raw * half_scale)).astype(BF16)

    def slab(u):
        return w[u].reshape(WIDTH, PAIR)

    def feed_up(j):
        raw[...] = jnp.dot(normed[...], slab(U_FF + 2 * j), preferred_element_type=F32)

    def feed_gate(j):
        columns = block_of(j)
        for s in range(SEQS):
            some = slice(s * LENGTH, (s + 1) * LENGTH)
            raw[some, :] = activation(raw[some, :], columns)
        gate_raw = jnp.dot(normed[...], slab(U_FF + 2 * j + 1), preferred_element_type=F32)
        hid[:, columns] = hidden_of(raw[...], gate_raw, columns)

    def feed_last(_):
        both = jnp.dot(normed[...], slab(U_LAST), preferred_element_type=F32)
        columns = pl.ds(10 * LANES, LANES)
        for s in range(SEQS):
            some = slice(s * LENGTH, (s + 1) * LENGTH)
            active = activation(both[some, :LANES], columns)
            hid[some, columns] = hidden_of(active, both[some, LANES:], columns)

    def down_first(n):
        side, block = n // 4, lax.rem(n, 4)
        right = jnp.concatenate(
            [w[u, side, block].reshape(256, PAIR) for u in range(U_DOWN, U_TILE)], axis=1
        )
        acc[:, block_of(n)] = dot_nt(hid[:, 0:FIRST], right)

    def down_rest(side, block):
        right = jnp.concatenate(
            [w_tile[k, side, block].reshape(256, LANES) for k in range(TILES)], axis=1
        )
        return acc[:, block_of(side * 4 + block)] + dot_nt(hid[:, FIRST:HID], right)

    def compute(m):
        start = 0
        starts = {}
        for name, count in PIECES:
            starts[name] = (start, count)
            start += count

        def during(name, body):
            first_one, count = starts[name]

            @pl.when((m >= first_one) & (m < first_one + count))
            def _():
                body(m - first_one)

        def share(_):
            across(x_hbm, x.at[tp], X_INPUT).start()
            across(gain_hbm, mate_gain, X_GAIN).start()
            across(out_scale_hbm, mate_out_scale, X_SCALE).start()

        def pooling(s):
            @pl.when(s == 0)
            def _():
                for load in loads[5:]:
                    load.wait()
                across(x_hbm, x.at[mate], X_INPUT).wait_recv()
                across(gain_hbm, mate_gain, X_GAIN).wait_recv()
                across(out_scale_hbm, mate_out_scale, X_SCALE).wait_recv()

            pool(s)

        def norming(s):
            @pl.when(s == 0)
            def _():
                across(part, got, X_MIXER).wait_recv()

            norm(s)

        def feeding(k):
            @pl.when(lax.rem(k, 2) == 0)
            def _():
                feed_up(k // 2)

            @pl.when(lax.rem(k, 2) == 1)
            def _():
                feed_gate(k // 2)

        during("share", share)
        during("pool", pooling)
        during("group", group)
        during("project half", project_half)
        during("project", project_rest)
        during("norm", norming)
        during("last", feed_last)
        again = starts["feed again"][0]
        early, late = (m >= starts["feed"][0]) & (m < starts["down"][0]), m >= again

        @pl.when(early | late)
        def _():
            feeding(jnp.where(late, m - again + starts["feed"][1], m - starts["feed"][0]))

        during("down", down_first)

    def micro(m, _):
        def among(low, high):
            if high - low == 1:
                gather(low)
                return
            half = (low + high) // 2
            pl.when(m < half)(lambda: among(low, half))
            pl.when(m >= half)(lambda: among(half, high))

        among(0, TOTAL)
        compute(m)
        return 0

    lax.fori_loop(0, TOTAL, micro, 0)
    gather(TOTAL)

    across(part, got, X_MIXER).wait_send()

    def first_half(block, _):
        part[mate, :, block_of(block)] = down_rest(mate, block).astype(BF16)
        final_piece(block).start()
        return 0

    lax.fori_loop(0, 4, first_half, 0)

    def second_half(block, _):
        columns = block_of(block)
        final_piece(block).wait_recv()
        total = down_rest(tp, block).astype(BF16).astype(F32) + end[:, columns].astype(F32)
        scale = down_scale[columns].reshape(1, PAIR)
        y[:, columns] = (mid[tp, :, columns].astype(F32) + total * scale).astype(BF16)
        return 0

    lax.fori_loop(0, 4, second_half, 0)

    across(x_hbm, x.at[tp], X_INPUT).wait_send()
    across(gain_hbm, mate_gain, X_GAIN).wait_send()
    across(out_scale_hbm, mate_out_scale, X_SCALE).wait_send()
    for block in range(4):
        final_piece(block).wait_send()
    full, over = divmod(U_TILE, SEND_GROUP)
    lanes = [2 * PAIR * SEND_GROUP] * full + [2 * PAIR * over, PAIR * TILES]
    for k in range(full + 2):
        ref = normed.at[pl.ds(0, 31 * 32), pl.ds(0, lanes[k])]
        pltpu.make_async_copy(ref, ref, send_sem.at[k]).wait()


def layer(
    layer_in,
    mix_gain,
    pool_weight,
    pool_scale,
    out_weight,
    out_scale,
    channel_gain,
    up_weight,
    up_scale,
    gate_weight,
    gate_scale,
    conv_weight,
    down_weight,
    down_scale,
):
    anywhere = pl.BlockSpec(memory_space=pl.ANY)
    dma = pltpu.SemaphoreType.DMA
    return pl.pallas_call(
        kernel,
        out_shape=pltpu.VMEM((ROWS, HALF), BF16),
        in_specs=[anywhere] * 14,
        out_specs=pl.BlockSpec(memory_space=pltpu.VMEM),
        scratch_shapes=[
            pltpu.VMEM((U_TILE, 2, 4, 4, 64, PAIR), BF16),
            pltpu.VMEM((TILES, 2, 4, 4, 64, LANES), BF16),
            pltpu.VMEM((2, ROWS, HALF), BF16),
            pltpu.VMEM((2, ROWS, HALF), BF16),
            pltpu.VMEM((2, ROWS, HALF), BF16),
            pltpu.VMEM((ROWS, HALF), BF16),
            pltpu.VMEM((2, ROWS, HALF), BF16),
            pltpu.VMEM((ROWS, WIDTH), BF16),
            pltpu.VMEM((ROWS, HID), BF16),
            pltpu.VMEM((ROWS, WIDTH), F32),
            pltpu.VMEM((ROWS, PAIR), F32),
            pltpu.VMEM((2, 16, 512), F32),
            pltpu.VMEM((64, HALF), F32),
            pltpu.VMEM((64, HID), F32),
            pltpu.VMEM((64, HID), F32),
            pltpu.VMEM((64, HID), F32),
            pltpu.VMEM((HALF,), BF16),
            pltpu.VMEM((2, 512), F32),
            pltpu.VMEM((HALF,), F32),
            pltpu.VMEM((HALF,), F32),
            pltpu.VMEM((HALF,), BF16),
            pltpu.VMEM((HALF,), BF16),
            pltpu.VMEM((HID,), F32),
            pltpu.VMEM((HID,), F32),
            pltpu.VMEM((3, HID), F32),
            pltpu.VMEM((HALF,), F32),
            dma((14,)),
            dma((group_of(U_TILE) + 1,)),
            dma((UNITS, STAGES)),
            dma((8,)),
            dma((8,)),
        ],
        compiler_params=pltpu.CompilerParams(
            collective_id=0, has_side_effects=True, vmem_limit_bytes=63_500_000
        ),
    )(
        layer_in,
        pool_weight.transpose(0, 2, 1),
        out_weight.T,
        up_weight,
        gate_weight,
        down_weight.T,
        mix_gain,
        pool_scale,
        out_scale,
        channel_gain,
        up_scale,
        gate_scale,
        conv_weight,
        down_scale,
    )


def solution(mesh):
    torus = Mesh(
        mesh.devices.reshape(mesh.shape["rep"], 2, 4, 4, mesh.shape["tp"]),
        ("rep", "fs_0", "fs_1", "fs_2", "tp"),
    )
    in_specs = (
        P(REP_FS, "tp"),
        P("tp"),
        P("tp", None, FS),
        P("tp", None),
        P("tp", FS),
        P("tp"),
        P("tp"),
        P(FS, "tp"),
        P("tp"),
        P(FS, "tp"),
        P("tp"),
        P(None, "tp"),
        P("tp", FS),
        P("tp"),
    )
    out_specs = P(REP_FS, "tp")
    return jax.shard_map(
        layer, mesh=torus, in_specs=in_specs, out_specs=out_specs, check_vma=False
    )
```
